32 devices in a mesh: sp: 8 (over z, x), dp: 4 (over y, core).
Axes of the slice: x: 2, y: 2, z: 4, core: 2. Of those that a mesh axis runs over, the one named last changes fastest.
Arguments:
- normed_input: bfloat16 [2560, 2048], P('sp'), may hold values from -6 to 6
- out_grad: bfloat16 [2560, 2048], P('sp'), may hold values from -6 to 6
- value_weight: bfloat16 [2048, 1024], P(None, 'dp'), may hold values from -0.125 to 0.125
- gate_weight: bfloat16 [2048, 1024], P(None, 'dp'), may hold values from -0.125 to 0.125
- down_weight: bfloat16 [1024, 2048], P('dp'), may hold values from -0.1875 to 0.1875
- conv_kernel: float32 [31, 1024], P(None, 'dp'), may hold values from -5 to 5
- conv_bias: float32 [1024], P('dp'), may hold values from -3 to 3
- norm_gain: float32 [1024], P('dp'), may hold values from 0.1 to 1.9
- norm_shift: float32 [1024], P('dp'), may hold values from -3 to 3
Outputs:
- input_grad: bfloat16 [2560, 2048], P('sp')
- value_grad: float32 [2048, 1024], P('sp', 'dp')
- gate_grad: float32 [2048, 1024], P('sp', 'dp')
- down_grad: float32 [1024, 2048], P('dp', 'sp')
- kernel_grad: float32 [31, 1024], P(None, 'dp')
- bias_grad: float32 [1024], P('dp')
- gain_grad: float32 [1024], P('dp')
- shift_grad: float32 [1024], P('dp')
The draws below stay inside these ranges and needn't reach their ends.
All inputs are finite; a program needn't handle non-finite values.
Results may differ from the reference program's by a relative error of at most 0.006.
Values may be sent and summed in bfloat16 or wider, within the bound.
A program may use at most 64 MiB of HBM per device.

```python
import math
import jax
import jax.numpy as jnp
from jax import lax

D = 2048
C = 1024
KW = 31
TOKENS = 2560


def draw_conv_kernel(key, part):
    first, second = jax.random.split(jax.random.fold_in(key, 11))
    place = jnp.arange(C, dtype=jnp.float32) / C
    jitter = jax.random.uniform(first, (C,), jnp.float32, -0.25, 0.25)
    scale = jnp.exp(jnp.log(0.5) + jnp.log(10.0) * place + jitter)
    base = jnp.clip(jax.random.normal(second, (KW, C), jnp.float32), -4.0, 4.0)
    return base * scale[None, :] / math.sqrt(KW)


def draw_conv_bias(key, part):
    noise_key = jax.random.fold_in(key, 23)
    place = jnp.arange(C, dtype=jnp.float32) / C
    noise = jnp.clip(jax.random.normal(noise_key, (C,), jnp.float32), -4.0, 4.0)
    return -0.8 + 2.0 * place + 0.4 * noise


def strengthened(array, key, source, target, blocks, factor):
    def block_of(dim):
        return (jnp.arange(array.shape[dim]) // (array.shape[dim] // blocks)).reshape((-1,) + (1,) * (array.ndim - 1 - dim))

    one_side = jax.random.permutation(key, blocks)[block_of(target)]
    second = (block_of(target) + blocks // 2) % blocks
    return jnp.where((block_of(source) == one_side) | (block_of(source) == second), factor * array, array)


def steps_of(key, shape, shards, least, high):
    gain, own = 1.0, jax.random.fold_in(key, 6)
    for axis_at, blocks in shards:
        draws = jnp.exp(jax.random.uniform(jax.random.fold_in(own, axis_at), (blocks,), jnp.float32, least / len(shards), high / len(shards)))
        gain = gain * jnp.repeat(draws, shape[axis_at] // blocks).reshape([-1 if axis == axis_at else 1 for axis in range(len(shape))])
    return gain


def bell_draw(rng, shape, scale, bound, cuts=(), kind=jnp.bfloat16):
    values = scale * jax.random.normal(rng, shape, jnp.float32)
    if cuts:
        values = values * steps_of(rng, shape, cuts, -0.22, 0.18)
    return jnp.clip(values, -bound, bound).astype(kind)


def heavy_noise(own_key, extent, scale, most, pieces, heavy, kind=jnp.bfloat16):
    values = scale * jax.random.normal(own_key, extent, jnp.float32)
    if pieces:
        values = values * steps_of(own_key, extent, pieces, -0.22, 0.18)
    return jnp.clip(strengthened(values, jax.random.fold_in(own_key, 3), *heavy), -most, most).astype(kind)


def setup_inputs(seed: int = 0) -> dict:
    keys = jax.random.split(jax.random.key(seed), 10)
    normed_input = heavy_noise(keys[0], (TOKENS, D), 1.0, 6.0, ((0, 8),), (0, 1, 8, 2.0))
    out_grad = heavy_noise(keys[1], (TOKENS, D), 1.0, 6.0, ((0, 8),), (0, 1, 8, 2.0))
    value_weight = bell_draw(keys[2], (D, C), D ** -0.5, 0.125, ((1, 4),))
    gate_weight = bell_draw(keys[3], (D, C), D ** -0.5, 0.125, ((1, 4),))
    down_weight = bell_draw(keys[4], (C, D), C ** -0.5, 0.1875, ((0, 4),))
    conv_kernel = draw_conv_kernel(jax.random.fold_in(keys[9], 71), 0)
    conv_bias = draw_conv_bias(jax.random.fold_in(keys[9], 71), 0)
    norm_gain = jnp.clip(1.0 + 0.18 * jax.random.normal(keys[7], (C,), jnp.float32), 0.1, 1.9)
    norm_shift = bell_draw(keys[8], (C,), 0.5, 3.0, ((0, 4),), jnp.float32)
    return {"normed_input": normed_input, "out_grad": out_grad, "value_weight": value_weight, "gate_weight": gate_weight, "down_weight": down_weight, "conv_kernel": conv_kernel, "conv_bias": conv_bias, "norm_gain": norm_gain, "norm_shift": norm_shift}


EPS = 1e-05

def reference(normed_input, out_grad, value_weight, gate_weight, down_weight, conv_kernel, conv_bias, norm_gain, norm_shift):
    reach = KW // 2
    ratio = 1.0 / math.sqrt(TOKENS)
    value_b = jnp.dot(normed_input, value_weight, preferred_element_type=jnp.float32).astype(jnp.bfloat16)
    gate_b = jnp.dot(normed_input, gate_weight, preferred_element_type=jnp.float32).astype(jnp.bfloat16)
    value = lax.optimization_barrier(value_b).astype(jnp.float32)
    gate = lax.optimization_barrier(gate_b).astype(jnp.float32)
    opening = jax.nn.sigmoid(gate)
    glu = value * opening
    padded = jnp.pad(glu, ((reach, reach), (0, 0)))
    mixed = jnp.zeros_like(glu) + conv_bias[None, :]
    for tap in range(KW):
        mixed = mixed + conv_kernel[tap][None, :] * padded[tap:tap + TOKENS]
    mean = lax.optimization_barrier(jnp.mean(mixed, axis=1, keepdims=True))
    spread = lax.optimization_barrier(jnp.mean((mixed - mean) * (mixed - mean), axis=1, keepdims=True))
    inv_std = lax.rsqrt(spread + EPS)
    centred = (mixed - mean) * inv_std
    normed = centred * norm_gain[None, :] + norm_shift[None, :]
    sig = jax.nn.sigmoid(normed)
    activated = (normed * sig).astype(jnp.bfloat16)
    d_act = jnp.dot(out_grad, down_weight.T, preferred_element_type=jnp.float32)
    d_normed = d_act * sig * (1.0 + normed * (1.0 - sig))
    d_centred = d_normed * norm_gain[None, :]
    first = lax.optimization_barrier(jnp.mean(d_centred, axis=1, keepdims=True))
    second = lax.optimization_barrier(jnp.mean(d_centred * centred, axis=1, keepdims=True))
    d_mixed = inv_std * (d_centred - first - centred * second)
    d_padded = jnp.pad(d_mixed, ((reach, reach), (0, 0)))
    d_glu = jnp.zeros_like(d_mixed)
    for tap in range(KW):
        d_glu = d_glu + conv_kernel[tap][None, :] * d_padded[2 * reach - tap:2 * reach - tap + TOKENS]
    kernel_grad = jnp.stack([lax.optimization_barrier(jnp.sum(d_mixed * padded[tap:tap + TOKENS], axis=0)) for tap in range(KW)]) * ratio
    bias_grad = lax.optimization_barrier(jnp.sum(d_mixed, axis=0)) * ratio
    gain_grad = lax.optimization_barrier(jnp.sum(d_normed * centred, axis=0)) * ratio
    shift_grad = lax.optimization_barrier(jnp.sum(d_normed, axis=0)) * ratio
    d_value = (d_glu * opening).astype(jnp.bfloat16)
    d_gate = (d_glu * value * opening * (1.0 - opening)).astype(jnp.bfloat16)
    value_grad = jnp.dot(normed_input.T, d_value, preferred_element_type=jnp.float32) * ratio
    gate_grad = jnp.dot(normed_input.T, d_gate, preferred_element_type=jnp.float32) * ratio
    down_grad = jnp.dot(activated.T, out_grad, preferred_element_type=jnp.float32) * ratio
    input_grad = (jnp.dot(d_value, value_weight.T, preferred_element_type=jnp.float32) + jnp.dot(d_gate, gate_weight.T, preferred_element_type=jnp.float32)).astype(jnp.bfloat16)
    return (input_grad, value_grad, gate_grad, down_grad, kernel_grad, bias_grad, gain_grad, shift_grad)
```

```python
import functools
import math

import jax
import jax.numpy as jnp
from jax import lax
from jax.experimental import pallas as pl
from jax.experimental.pallas import tpu as pltpu
from jax.sharding import PartitionSpec as P

EPS = 1e-05
F32 = jnp.float32
BF16 = jnp.bfloat16
MESH = pl.DeviceIdType.MESH
NN = (((1,), (0,)), ((), ()))
NT = (((1,), (1,)), ((), ()))
TN = (((0,), (0,)), ((), ()))
PAD = 16
ROWS = 32
SUBS = 2
GROUPS = 4
MAIN = 61_900_000
FINISH = 16_000_000


def dot(a, b, numbers):
    return lax.dot_general(a, b, numbers, preferred_element_type=F32)


def split3(v):
    high = v.astype(BF16)
    rest = v - high.astype(F32)
    mid = rest.astype(BF16)
    return high, mid, (rest - mid.astype(F32)).astype(BF16)


def is_wide(chunk, chans):
    return chunk % 128 == 0 and chans % 32 == 0


def kernel(
    sp,
    dp,
    ratio,
    x_hbm,
    og_hbm,
    wv_hbm,
    wg_hbm,
    wd_hbm,
    ck_hbm,
    bias_hbm,
    gain_hbm,
    shift_hbm,
    ig_out,
    vg_out,
    gg_out,
    dg_out,
    small_out,
    x,
    og,
    wv,
    wg,
    wd,
    ck,
    bias,
    gain,
    shift,
    load_sem,
    value,
    opening,
    glu,
    mixed,
    d_act,
    d_pad,
    act,
    dv,
    dg,
    turned,
    cols,
    stats,
    stats2,
    part,
    ring_src,
    ring_dst,
    ig_send,
    ig_recv,
    ig_own,
    ig_sum,
    ig_peer,
    small,
    small_recv,
    halo_send,
    halo_recv,
    stat_send,
    stat_recv,
    ring_send,
    ring_recv,
    ig_ssem,
    ig_rsem,
    small_ssem,
    small_rsem,
):
    tokens, width = x.shape
    taps, chans = ck.shape
    channels = chans * dp
    reach = taps // 2
    chunk = width // sp
    wide = is_wide(chunk, chans)
    lines = chans if wide else chunk
    strip = lines // (2 * SUBS)
    tile = min(256, width)
    s = lax.axis_index("sp")
    d = lax.axis_index("dp")
    bits_sp = sp.bit_length() - 1
    bits_dp = dp.bit_length() - 1

    def flip(i, bit):
        step = 1 << bit
        return i + step * (1 - 2 * lax.rem(lax.div(i, step), 2))

    def index_of(p):
        far = lax.div(p, sp // 2)
        return (1 - far) * 2 * p + far * (2 * sp - 1 - 2 * p)

    odd = lax.rem(s, 2)
    pos = (1 - odd) * lax.div(s, 2) + odd * (sp - 1 - lax.div(s, 2))
    ahead = index_of(lax.rem(pos + 1, sp))
    behind = index_of(lax.rem(pos + sp - 1, sp))

    loads = [
        pltpu.make_async_copy(src, dst, load_sem.at[at])
        for at, (src, dst) in enumerate(
            [
                (x_hbm, x),
                (wv_hbm, wv),
                (wg_hbm, wg),
                (og_hbm, og),
                (wd_hbm, wd),
                (ck_hbm, ck),
                (bias_hbm, bias),
                (gain_hbm, gain),
                (shift_hbm, shift),
            ]
        )
    ]
    for load in loads:
        load.start()

    barrier = pltpu.get_barrier_semaphore()
    peers = [ahead, behind, lax.rem(s + 1, sp), lax.rem(s + sp - 1, sp)]
    peers += [flip(s, bit) for bit in range(bits_sp)]
    for peer in peers:
        pl.semaphore_signal(barrier, inc=1, device_id={"sp": peer}, device_id_type=MESH)
    for off in range(1, dp):
        pl.semaphore_signal(
            barrier, inc=1, device_id={"dp": lax.rem(d + off, dp)}, device_id_type=MESH
        )

    loads[0].wait()
    loads[1].wait()
    value[...] = dot(x[...], wv[...], NN).astype(BF16).astype(F32)
    loads[2].wait()
    opening[...] = dot(x[...], wg[...], NN).astype(BF16).astype(F32)

    def row_loop(fn, init=None, rows=ROWS):
        def step(i, carry):
            return fn(pl.multiple_of(i * rows, rows), carry)

        return lax.fori_loop(0, tokens // rows, step, init)

    big = 80 if tokens % 80 == 0 else ROWS

    def make_glu(r, _):
        here = pl.ds(r, ROWS)
        o = jax.nn.sigmoid(opening[here, :])
        opening[here, :] = o
        glu[pl.ds(r + PAD, ROWS), :] = value[here, :] * o

    row_loop(make_glu)
    pl.semaphore_wait(barrier, len(peers) + dp - 1)

    has_low, has_high = s > 0, s < sp - 1

    def halo_copies(buf, at):
        up = pltpu.make_async_remote_copy(
            src_ref=buf.at[pl.ds(tokens, PAD)],
            dst_ref=buf.at[pl.ds(0, PAD)],
            send_sem=halo_send.at[at],
            recv_sem=halo_recv.at[at],
            device_id={"sp": lax.rem(s + 1, sp)},
            device_id_type=MESH,
        )
        down = pltpu.make_async_remote_copy(
            src_ref=buf.at[pl.ds(PAD, PAD)],
            dst_ref=buf.at[pl.ds(tokens + PAD, PAD)],
            send_sem=halo_send.at[at + 1],
            recv_sem=halo_recv.at[at + 1],
            device_id={"sp": lax.rem(s + sp - 1, sp)},
            device_id_type=MESH,
        )
        return up, down

    def halo_start(buf, at):
        up, down = halo_copies(buf, at)
        pl.when(has_high)(up.start)
        pl.when(has_low)(down.start)

        @pl.when(s == 0)
        def _():
            buf[pl.ds(0, PAD), :] = jnp.zeros((PAD, chans), F32)

        @pl.when(s == sp - 1)
        def _():
            buf[pl.ds(tokens + PAD, PAD), :] = jnp.zeros((PAD, chans), F32)

    def halo_wait(buf, at):
        up, down = halo_copies(buf, at)

        @pl.when(has_low)
        def _():
            up.wait_recv()
            down.wait_send()

        @pl.when(has_high)
        def _():
            down.wait_recv()
            up.wait_send()

    def inner_outer(fn, between):
        blocks = tokens // ROWS

        def inner(i, _):
            fn(pl.multiple_of(i * ROWS, ROWS), None)

        def outer(i, _):
            fn(pl.multiple_of(i * (blocks - 1) * ROWS, ROWS), None)

        lax.fori_loop(1, blocks - 1, inner, None)
        between()
        lax.fori_loop(0, 2, outer, None)

    halo_start(glu, 0)
    for load in loads[3:]:
        load.wait()
    d_act[...] = dot(og[...], wd[...], NT)

    span = ROWS + 2 * PAD

    def shifted(buf, r, offset):
        window = buf[pl.ds(r, span), :]
        return pltpu.roll(window, span - offset, 0) if offset else window

    def slide(buf, r, offset_of, acc):
        for low in range(8):
            those = [tap for tap in range(taps) if offset_of(tap) % 8 == low]
            if those:
                window = shifted(buf, r, low)
                for tap in those:
                    high = offset_of(tap) - low
                    acc = acc + ck[tap : tap + 1, :] * window[high : high + ROWS]
        return acc

    def conv(r, _):
        acc = jnp.zeros((ROWS, chans), F32) + bias[...]
        mixed[pl.ds(r, ROWS), :] = slide(glu, r, lambda tap: tap + PAD - reach, acc)

    inner_outer(conv, lambda: halo_wait(glu, 0))

    ones = jnp.ones((16, chans), BF16)
    line = lax.broadcasted_iota(jnp.int32, (8, tokens), 0)
    eye = (
        lax.rem(lax.broadcasted_iota(jnp.int32, (24, 128), 0), 8)
        == lax.broadcasted_iota(jnp.int32, (24, 128), 1)
    ).astype(BF16)
    pieces = [(at, min(128, tokens - at)) for at in range(0, tokens, 128)]

    def row_sums(v):
        a, b, c = (dot(ones, term, NT) for term in split3(v))
        return a + b + c

    def columns(one, two):
        both = jnp.where(line == 0, one, jnp.where(line == 1, two, 0.0))
        terms = [term.astype(F32) for term in split3(both)]
        return dot(jnp.concatenate(terms, axis=0).astype(BF16), eye, TN)

    def stat_copy(buf, off, at):
        return pltpu.make_async_remote_copy(
            src_ref=buf.at[0],
            dst_ref=buf.at[off],
            send_sem=stat_send.at[at * dp + off],
            recv_sem=stat_recv.at[at * dp + off],
            device_id={"dp": lax.rem(d + off, dp)},
            device_id_type=MESH,
        )

    def stat_start(buf, at, one, two):
        buf[0] = jnp.zeros(buf.shape[1:], F32)
        for first, sums in ((0, row_sums(one)), (len(pieces), row_sums(two))):
            for j, (begin, size) in enumerate(pieces):
                buf[0, first + j : first + j + 1, 0:size] = sums[0:1, begin : begin + size]
        for off in range(1, dp):
            stat_copy(buf, off, at).start()

    def stat_wait(buf, at):
        for off in range(1, dp):
            stat_copy(buf, off, at).wait()
        total = buf[0]
        for off in range(1, dp):
            total = total + buf[off]
        total = total * (1.0 / channels)
        one, two = (
            jnp.concatenate(
                [total[first + j : first + j + 1, 0:size] for j, (_, size) in enumerate(pieces)],
                axis=1,
            )
            for first in (0, len(pieces))
        )
        return one, two

    stat_start(stats, 0, mixed[...], mixed[...] * mixed[...])
    mean, square = stat_wait(stats, 0)
    cols[0] = columns(mean, lax.rsqrt(square - mean * mean + EPS))

    def norm(r, carry):
        gain_sum, shift_sum = carry
        here = pl.ds(r, big)
        col = cols[0, here, :]
        centred = (mixed[here, :] - col[:, 0:1]) * col[:, 1:2]
        normed = centred * gain[...] + shift[...]
        sig = jax.nn.sigmoid(normed)
        act[here, :] = (normed * sig).astype(BF16)
        d_normed = d_act[here, :] * sig * (1.0 + normed * (1.0 - sig))
        mixed[here, :] = centred
        d_act[here, :] = d_normed * gain[...]
        gain_sum = gain_sum + jnp.sum(d_normed * centred, axis=0, keepdims=True)
        shift_sum = shift_sum + jnp.sum(d_normed, axis=0, keepdims=True)
        return gain_sum, shift_sum

    zero = jnp.zeros((1, chans), F32)
    gain_sum, shift_sum = row_loop(norm, (zero, zero), big)
    stat_start(stats2, 1, d_act[...], d_act[...] * mixed[...])

    def several(count, fn):
        if count <= 8:
            for i in range(count):
                fn(i)
        else:
            lax.fori_loop(0, count, lambda i, _: fn(i), None)

    def grad_tile(at, rows, off):
        index = index_of(lax.rem(pos + off + 2 * sp, sp))
        those = pl.ds(pl.multiple_of(index * chunk, chunk), chunk)
        part[at, pl.ds(pl.multiple_of(index * lines, lines), lines), :] = dot(
            turned[at], rows[:, those], NN
        )

    def grad_first(at, rows, factor):
        if wide:
            turned[at] = factor[...].T
            grad_tile(at, rows, -1)
            grad_tile(at, rows, 1)
            return

        def step(i, _):
            here = pl.ds(pl.multiple_of(i * tile, tile), tile)
            part[at, here, :] = dot(rows[:, here], factor[...], TN)

        lax.fori_loop(0, width // tile, step, None)

    def grad_rest(at, rows):
        if wide:
            several(sp - 2, lambda i: grad_tile(at, rows, (i + 2) % (sp - 1)))

    streams = [
        (at, 2 * sub + (way < 0), way) for at in range(3) for sub in range(SUBS) for way in (1, -1)
    ]
    early = [i for i, (at, _, _) in enumerate(streams) if at == 2]
    late = [i for sub in range(SUBS) for i, (at, place, _) in enumerate(streams) if at < 2 and place // 2 == sub]

    def late_of(at):
        return [i for i in late if streams[i][0] == at]

    def piece(stream, p):
        at, place, _ = streams[stream]
        first = index_of(lax.rem(p + 2 * sp, sp)) * lines + place * strip
        return part[at, pl.ds(pl.multiple_of(first, strip), strip), :]

    def ring_copy(stream, k):
        return pltpu.make_async_remote_copy(
            src_ref=ring_src.at[stream, k],
            dst_ref=ring_dst.at[stream, k],
            send_sem=ring_send.at[stream, k],
            recv_sem=ring_recv.at[stream, k],
            device_id={"sp": ahead if streams[stream][2] == 1 else behind},
            device_id_type=MESH,
        )

    def ring_step(k, which):
        for stream in which:
            way = streams[stream][2]
            mine = piece(stream, pos - way * (1 + k))
            if not (isinstance(k, int) and k == 0):
                ring_copy(stream, k - 1).wait_recv()
                mine = mine + ring_dst[stream, k - 1].astype(F32)
            ring_src[stream, k] = mine.astype(BF16)
            ring_copy(stream, k).start()

    def ring_end(which, outs):
        for stream in which:
            at, place, _ = streams[stream]
            ring_copy(stream, sp - 2).wait_recv()
            outs[at][pl.ds(place * strip, strip), :] = ratio * (
                piece(stream, pos) + ring_dst[stream, sp - 2].astype(F32)
            )

    grad_first(2, og, act)
    ring_step(0, early)
    grad_rest(2, og)

    first, second = stat_wait(stats2, 1)
    cols[1] = columns(first, second)

    def norm_back(r, bias_sum):
        here = pl.ds(r, big)
        col, back = cols[0, here, :], cols[1, here, :]
        d_mixed = col[:, 1:2] * (d_act[here, :] - back[:, 0:1] - mixed[here, :] * back[:, 1:2])
        d_pad[pl.ds(r + PAD, big), :] = d_mixed
        return bias_sum + jnp.sum(d_mixed, axis=0, keepdims=True)

    bias_sum = row_loop(norm_back, zero, big)
    halo_start(d_pad, 2)
    ring_step(1, early)

    def conv_back(r, _):
        here = pl.ds(r, ROWS)
        acc = jnp.zeros((ROWS, chans), F32)
        acc = slide(d_pad, r, lambda tap: PAD + reach - tap, acc)
        o = opening[here, :]
        grad = acc * o
        dv[here, :] = grad.astype(BF16)
        dg[here, :] = (grad * value[here, :] * (1.0 - o)).astype(BF16)

    inner_outer(conv_back, lambda: halo_wait(d_pad, 2))
    grad_first(0, x, dv)
    ring_step(0, late_of(0))
    grad_first(1, x, dg)
    ring_step(0, late_of(1))
    grad_rest(0, x)
    grad_rest(1, x)
    ring_step(2, early)

    half = tokens // 2
    mine = pl.multiple_of(lax.rem(d, 2) * half, half)
    other = pl.multiple_of((1 - lax.rem(d, 2)) * half, half)
    group = width // GROUPS

    def ig_copy(at, g, src, dst, bit):
        return pltpu.make_async_remote_copy(
            src_ref=src,
            dst_ref=dst,
            send_sem=ig_ssem.at[at, g],
            recv_sem=ig_rsem.at[at, g],
            device_id={"dp": flip(d, bit)},
            device_id_type=MESH,
        )

    def of_group(g):
        return pl.ds(g * group, group)

    def pair_copy(g):
        return ig_copy(0, g, ig_send.at[:, of_group(g)], ig_recv.at[:, of_group(g)], 0)

    def y_copy(bit, g):
        return ig_copy(
            bit, g, ig_sum.at[bit - 1, :, of_group(g)], ig_peer.at[bit - 1, :, of_group(g)], bit
        )

    final = bits_dp - 1

    def give_copy(g):
        return ig_copy(
            bits_dp,
            g,
            ig_sum.at[final, :, of_group(g)],
            ig_out.at[pl.ds(mine, half), of_group(g)],
            0,
        )

    both_v = jnp.concatenate([dv[pl.ds(other, half), :], dv[pl.ds(mine, half), :]], axis=0)
    both_g = jnp.concatenate([dg[pl.ds(other, half), :], dg[pl.ds(mine, half), :]], axis=0)
    size = min(tile, group)
    for g in range(GROUPS):
        for begin in range(g * group, (g + 1) * group, size):
            here = pl.ds(begin, size)
            got = dot(both_v, wv[here, :], NT) + dot(both_g, wg[here, :], NT)
            ig_send[:, here] = got[:half].astype(BF16)
            ig_own[:, here] = got[half:]
        pair_copy(g).start()

    def pair_sums():
        for g in range(GROUPS):
            pair_copy(g).wait_recv()
            here = of_group(g)
            ig_sum[0, :, here] = (ig_own[:, here] + ig_recv[:, here].astype(F32)).astype(BF16)
            if bits_dp > 1:
                y_copy(1, g).start()

    small[0] = jnp.zeros(small.shape[1:], F32)

    def taps_grad(low):
        those = [
            [tap for tap in range(taps) if (tap + PAD - reach) % 8 == low + at] for at in range(2)
        ]

        def taps_sum(r, sums):
            grad = d_pad[pl.ds(r + PAD, ROWS), :]
            new = []
            for at in range(2):
                window = shifted(glu, r, low + at)
                for tap in those[at]:
                    high = tap + PAD - reach - low - at
                    prod = grad * window[high : high + ROWS]
                    acc = sums[len(new)]
                    for row in range(0, ROWS, 8):
                        acc = acc + prod[row : row + 8]
                    new.append(acc)
            return tuple(new)

        flat = those[0] + those[1]
        sums = row_loop(taps_sum, tuple(jnp.zeros((8, chans), F32) for _ in flat))
        for acc, tap in zip(sums, flat):
            small[0, tap : tap + 1, :] = jnp.sum(acc, axis=0, keepdims=True) * ratio

    def small_copy(bit):
        return pltpu.make_async_remote_copy(
            src_ref=small.at[bit],
            dst_ref=small_recv.at[bit],
            send_sem=small_ssem.at[bit],
            recv_sem=small_rsem.at[bit],
            device_id={"sp": flip(s, bit)},
            device_id_type=MESH,
        )

    def small_first():
        small[0, taps : taps + 1, :] = bias_sum * ratio
        small[0, taps + 1 : taps + 2, :] = gain_sum * ratio
        small[0, taps + 2 : taps + 3, :] = shift_sum * ratio
        small_copy(0).start()

    def small_next(bit):
        if bit < bits_sp:
            small_copy(bit).wait_recv()
            small[bit + 1] = small[bit] + small_recv[bit]
            if bit + 1 < bits_sp:
                small_copy(bit + 1).start()

    def taps_half(lows):
        for low in lows:
            taps_grad(low)

    pair_sums()
    fixed = min(sp - 2, 6)
    for k in range(1, fixed + 1):
        ring_step(k, late)
        if k + 2 <= sp - 2:
            ring_step(k + 2, early)
        if k == 1:
            taps_half((0, 2))
        if k == 2:
            taps_half((4, 6))
            small_first()
        if k > 2:
            small_next(k - 3)
    for bit in range(max(fixed - 2, 0), bits_sp):
        small_next(bit)
    if sp - 2 > fixed:

        def both(k, _):
            ring_step(k, late)
            ring_step(k + 2, early)

        lax.fori_loop(fixed + 1, sp - 3, both, None)
        ring_step(sp - 3, late)
        ring_step(sp - 2, late)

    for bit in range(1, bits_dp):
        for g in range(GROUPS):
            y_copy(bit, g).wait_recv()
            here = of_group(g)
            got = ig_sum[bit - 1, :, here].astype(F32) + ig_peer[bit - 1, :, here].astype(F32)
            ig_sum[bit, :, here] = got.astype(BF16)
            if bit + 1 < bits_dp:
                y_copy(bit + 1, g).start()
            else:
                give_copy(g).start()
    if bits_dp == 1:
        for g in range(GROUPS):
            give_copy(g).start()
    ig_out[pl.ds(mine, half), :] = ig_sum[final]
    small_out[...] = small[bits_sp]
    ring_end(early + late, (vg_out, gg_out, dg_out))

    for g in range(GROUPS):
        pair_copy(g).wait_send()
        for bit in range(1, bits_dp):
            y_copy(bit, g).wait_send()
        give_copy(g).wait()
    for bit in range(bits_sp):
        small_copy(bit).wait_send()

    def drain(k, _):
        for stream in early + late:
            ring_copy(stream, k).wait_send()

    lax.fori_loop(0, sp - 1, drain, None)


def finish(
    wide, ig, vg, gg, dgrad, small, ig_o, vg_o, gg_o, dg_o, k_o, b_o, g_o, s_o,
    t0, t1, k_v, b_v, g_v, s_v, sem,
):
    copies = []

    def send(src, dst):
        copies.append(pltpu.make_async_copy(src, dst, sem.at[len(copies)]))
        copies[-1].start()

    send(ig, ig_o)
    turn = [(vg, vg_o), (gg, gg_o)] if wide else [(dgrad, dg_o)]
    keep = [(dgrad, dg_o)] if wide else [(vg, vg_o), (gg, gg_o)]
    for src, dst in keep:
        send(src, dst)
    taps = k_o.shape[0]
    k_v[...] = small[0:taps, :]
    send(k_v, k_o)
    for at, (held, out) in enumerate(((b_v, b_o), (g_v, g_o), (s_v, s_o))):
        held[...] = small[taps + at, :]
        send(held, out)
    for (src, dst), held in zip(turn, (t0, t1)):
        held[...] = src[...].T
        send(held, dst)
    for copy in copies:
        copy.wait()


def on_device(
    normed_input,
    out_grad,
    value_weight,
    gate_weight,
    down_weight,
    conv_kernel,
    conv_bias,
    norm_gain,
    norm_shift,
):
    tokens, width = normed_input.shape
    taps, chans = conv_kernel.shape
    sp, dp = lax.axis_size("sp"), lax.axis_size("dp")
    ratio = 1.0 / math.sqrt(tokens * sp)
    chunk = width // sp
    bits_sp, bits_dp = sp.bit_length() - 1, dp.bit_length() - 1
    small_rows = -(-(taps + 3) // 8) * 8
    half = tokens // 2
    full = (tokens, chans)
    vmem = pl.BlockSpec(memory_space=pltpu.VMEM)
    hbm = pl.BlockSpec(memory_space=pltpu.HBM)
    dma = pltpu.SemaphoreType.DMA
    wide = is_wide(chunk, chans)
    lines, lanes = (chans, chunk) if wide else (chunk, chans)
    stat_rows = -(-2 * -(-tokens // 128) // 8) * 8
    count = 3 * 2 * SUBS
    ig, vg, gg, dgrad, small = pl.pallas_call(
        functools.partial(kernel, sp, dp, ratio),
        out_shape=(
            pltpu.VMEM((tokens, width), BF16),
            pltpu.VMEM((lines, lanes), F32),
            pltpu.VMEM((lines, lanes), F32),
            pltpu.VMEM((lines, lanes), F32),
            pltpu.VMEM((small_rows, chans), F32),
        ),
        in_specs=[hbm] * 9,
        out_specs=(vmem,) * 5,
        scratch_shapes=[
            pltpu.VMEM((tokens, width), BF16),
            pltpu.VMEM((tokens, width), BF16),
            pltpu.VMEM((width, chans), BF16),
            pltpu.VMEM((width, chans), BF16),
            pltpu.VMEM((chans, width), BF16),
            pltpu.VMEM((taps, chans), F32),
            pltpu.VMEM((1, chans), F32),
            pltpu.VMEM((1, chans), F32),
            pltpu.VMEM((1, chans), F32),
            dma((9,)),
            pltpu.VMEM(full, F32),
            pltpu.VMEM(full, F32),
            pltpu.VMEM((tokens + 2 * PAD, chans), F32),
            pltpu.VMEM(full, F32),
            pltpu.VMEM(full, F32),
            pltpu.VMEM((tokens + 2 * PAD, chans), F32),
            pltpu.VMEM(full, BF16),
            pltpu.VMEM(full, BF16),
            pltpu.VMEM(full, BF16),
            pltpu.VMEM((3, chans, tokens), BF16),
            pltpu.VMEM((2, tokens, 128), F32),
            pltpu.VMEM((dp, stat_rows, 128), F32),
            pltpu.VMEM((dp, stat_rows, 128), F32),
            pltpu.VMEM((3, sp * lines, lanes), F32),
            pltpu.VMEM((count, sp - 1, lines // (2 * SUBS), lanes), BF16),
            pltpu.VMEM((count, sp - 1, lines // (2 * SUBS), lanes), BF16),
            pltpu.VMEM((half, width), BF16),
            pltpu.VMEM((half, width), BF16),
            pltpu.VMEM((half, width), F32),
            pltpu.VMEM((bits_dp, half, width), BF16),
            pltpu.VMEM((bits_dp - 1, half, width), BF16),
            pltpu.VMEM((bits_sp + 1, small_rows, chans), F32),
            pltpu.VMEM((bits_sp, small_rows, chans), F32),
            dma((4,)),
            dma((4,)),
            dma((2 * dp,)),
            dma((2 * dp,)),
            dma((count, sp - 1)),
            dma((count, sp - 1)),
            dma((bits_dp + 1, GROUPS)),
            dma((bits_dp + 1, GROUPS)),
            dma((bits_sp,)),
            dma((bits_sp,)),
        ],
        compiler_params=pltpu.CompilerParams(
            collective_id=0, has_side_effects=True, vmem_limit_bytes=MAIN
        ),
    )(
        normed_input,
        out_grad,
        value_weight,
        gate_weight,
        down_weight,
        conv_kernel,
        conv_bias[None, :],
        norm_gain[None, :],
        norm_shift[None, :],
    )
    row = jax.ShapeDtypeStruct((chans,), F32)
    return pl.pallas_call(
        functools.partial(finish, wide),
        out_shape=(
            jax.ShapeDtypeStruct(ig.shape, BF16),
            jax.ShapeDtypeStruct(vg.shape, F32),
            jax.ShapeDtypeStruct(gg.shape, F32),
            jax.ShapeDtypeStruct((chans, chunk), F32),
            jax.ShapeDtypeStruct((taps, chans), F32),
            row,
            row,
            row,
        ),
        in_specs=[vmem] * 5,
        out_specs=(hbm,) * 8,
        scratch_shapes=[
            pltpu.VMEM((lanes, lines), F32),
            pltpu.VMEM((lanes, lines), F32),
            pltpu.VMEM((taps, chans), F32),
            pltpu.VMEM((chans,), F32),
            pltpu.VMEM((chans,), F32),
            pltpu.VMEM((chans,), F32),
            dma((8,)),
        ],
        compiler_params=pltpu.CompilerParams(vmem_limit_bytes=FINISH),
    )(ig, vg, gg, dgrad, small)


def solution(mesh):
    in_specs = (
        P("sp", None),
        P("sp", None),
        P(None, "dp"),
        P(None, "dp"),
        P("dp", None),
        P(None, "dp"),
        P("dp"),
        P("dp"),
        P("dp"),
    )
    out_specs = (
        P("sp", None),
        P("sp", "dp"),
        P("sp", "dp"),
        P("dp", "sp"),
        P(None, "dp"),
        P("dp"),
        P("dp"),
        P("dp"),
    )
    return jax.shard_map(
        on_device, mesh=mesh, in_specs=in_specs, out_specs=out_specs, check_vma=False
    )
```

```python
import functools
import math

import jax
import jax.numpy as jnp
from jax import lax
from jax.experimental import pallas as pl
from jax.experimental.pallas import tpu as pltpu
from jax.sharding import PartitionSpec as P

EPS = 1e-05
F32 = jnp.float32
BF16 = jnp.bfloat16
MESH = pl.DeviceIdType.MESH
NN = (((1,), (0,)), ((), ()))
NT = (((1,), (1,)), ((), ()))
TN = (((0,), (0,)), ((), ()))
PAD = 16
ROWS = 32
SUBS = 2
GROUPS = 2
MAIN = 61_900_000
FINISH = 16_000_000


def dot(a, b, numbers):
    return lax.dot_general(a, b, numbers, preferred_element_type=F32)


def split3(v):
    high = v.astype(BF16)
    rest = v - high.astype(F32)
    mid = rest.astype(BF16)
    return high, mid, (rest - mid.astype(F32)).astype(BF16)


def is_wide(chunk, chans):
    return chunk % 128 == 0 and chans % 32 == 0


def kernel(
    sp,
    dp,
    ratio,
    x_hbm,
    og_hbm,
    wv_hbm,
    wg_hbm,
    wd_hbm,
    ck_hbm,
    bias_hbm,
    gain_hbm,
    shift_hbm,
    ig_out,
    vg_out,
    gg_out,
    dg_out,
    small_out,
    x,
    og,
    wv,
    wg,
    wd,
    ck,
    bias,
    gain,
    shift,
    load_sem,
    value,
    opening,
    glu,
    mixed,
    d_act,
    d_pad,
    act,
    dv,
    dg,
    turned,
    cols,
    stats,
    part,
    ring_src,
    ring_dst,
    ig_send,
    ig_recv,
    ig_own,
    ig_sum,
    ig_peer,
    small,
    small_recv,
    halo_send,
    halo_recv,
    stat_send,
    stat_recv,
    ring_send,
    ring_recv,
    ig_ssem,
    ig_rsem,
    give_rsem,
    small_ssem,
    small_rsem,
):
    tokens, width = x.shape
    taps, chans = ck.shape
    channels = chans * dp
    reach = taps // 2
    chunk = width // sp
    wide = is_wide(chunk, chans)
    lines = chans if wide else chunk
    strip = lines // (2 * SUBS)
    tile = min(256, width)
    s = lax.axis_index("sp")
    d = lax.axis_index("dp")
    bits_sp = sp.bit_length() - 1
    bits_dp = dp.bit_length() - 1

    def flip(i, bit):
        step = 1 << bit
        return i + step * (1 - 2 * lax.rem(lax.div(i, step), 2))

    def index_of(p):
        far = lax.div(p, sp // 2)
        return (1 - far) * 2 * p + far * (2 * sp - 1 - 2 * p)

    odd = lax.rem(s, 2)
    pos = (1 - odd) * lax.div(s, 2) + odd * (sp - 1 - lax.div(s, 2))
    ahead = index_of(lax.rem(pos + 1, sp))
    behind = index_of(lax.rem(pos + sp - 1, sp))

    loads = [
        pltpu.make_async_copy(src, dst, load_sem.at[at])
        for at, (src, dst) in enumerate(
            [
                (x_hbm, x),
                (wv_hbm, wv),
                (wg_hbm, wg),
                (og_hbm, og),
                (wd_hbm, wd),
                (ck_hbm, ck),
                (bias_hbm, bias),
                (gain_hbm, gain),
                (shift_hbm, shift),
            ]
        )
    ]
    for load in loads:
        load.start()

    barrier = pltpu.get_barrier_semaphore()
    peers = [ahead, behind, lax.rem(s + 1, sp), lax.rem(s + sp - 1, sp)]
    peers += [flip(s, bit) for bit in range(bits_sp)]
    for peer in peers:
        pl.semaphore_signal(barrier, inc=1, device_id={"sp": peer}, device_id_type=MESH)
    for off in range(1, dp):
        pl.semaphore_signal(
            barrier, inc=1, device_id={"dp": lax.rem(d + off, dp)}, device_id_type=MESH
        )

    for load in loads[:3]:
        load.wait()
    value_f, gate_f = dot(x[...], wv[...], NN), dot(x[...], wg[...], NN)
    value[...] = value_f.astype(BF16).astype(F32)
    opening[...] = gate_f.astype(BF16).astype(F32)

    def row_loop(fn, init=None, rows=ROWS, begin=0, end=tokens):
        def step(i, carry):
            return fn(pl.multiple_of(begin + i * rows, math.gcd(begin, rows)), carry)

        return lax.fori_loop(0, (end - begin) // rows, step, init)

    ext = tokens + 2 * PAD
    inner_rows = ext - 2 * ROWS
    big = 96 if inner_rows % 96 == 0 else ROWS
    own = pl.ds(PAD, tokens)

    def make_glu(r, _):
        here = pl.ds(r, ROWS)
        o = jax.nn.sigmoid(opening[here, :])
        opening[here, :] = o
        glu[pl.ds(r + 2 * PAD, ROWS), :] = value[here, :] * o

    row_loop(make_glu)
    pl.semaphore_wait(barrier, len(peers) + dp - 1)

    has_low, has_high = s > 0, s < sp - 1

    def halo_copies(buf, pad, at):
        up = pltpu.make_async_remote_copy(
            src_ref=buf.at[pl.ds(tokens, pad)],
            dst_ref=buf.at[pl.ds(0, pad)],
            send_sem=halo_send.at[at],
            recv_sem=halo_recv.at[at],
            device_id={"sp": lax.rem(s + 1, sp)},
            device_id_type=MESH,
        )
        down = pltpu.make_async_remote_copy(
            src_ref=buf.at[pl.ds(pad, pad)],
            dst_ref=buf.at[pl.ds(tokens + pad, pad)],
            send_sem=halo_send.at[at + 1],
            recv_sem=halo_recv.at[at + 1],
            device_id={"sp": lax.rem(s + sp - 1, sp)},
            device_id_type=MESH,
        )
        return up, down

    def halo_zero(buf, pad):
        @pl.when(s == 0)
        def _():
            buf[pl.ds(0, pad), :] = jnp.zeros((pad, chans), F32)

        @pl.when(s == sp - 1)
        def _():
            buf[pl.ds(tokens + pad, pad), :] = jnp.zeros((pad, chans), F32)

    def halo_start(buf, pad, at):
        up, down = halo_copies(buf, pad, at)
        pl.when(has_high)(up.start)
        pl.when(has_low)(down.start)
        halo_zero(buf, pad)

    def halo_wait(buf, pad, at):
        up, down = halo_copies(buf, pad, at)

        @pl.when(has_low)
        def _():
            up.wait_recv()
            down.wait_send()

        @pl.when(has_high)
        def _():
            down.wait_recv()
            up.wait_send()

    halo_start(glu, 2 * PAD, 0)
    for load in loads[3:]:
        load.wait()
    d_act[own, :] = dot(og[...], wd[...], NT)
    halo_start(d_act, PAD, 2)

    span = ROWS + 2 * PAD

    def shifted(buf, r, offset):
        window = buf[pl.ds(r, span), :]
        return pltpu.roll(window, span - offset, 0) if offset else window

    def slide(buf, r, offset_of, acc):
        for low in range(8):
            those = [tap for tap in range(taps) if offset_of(tap) % 8 == low]
            if those:
                window = shifted(buf, r, low)
                for tap in those:
                    high = offset_of(tap) - low
                    acc = acc + ck[tap : tap + 1, :] * window[high : high + ROWS]
        return acc

    def conv(r, _):
        acc = jnp.zeros((ROWS, chans), F32) + bias[...]
        mixed[pl.ds(r, ROWS), :] = slide(glu, r, lambda tap: tap + PAD - reach, acc)

    ones = jnp.ones((16, chans), BF16)
    eye = (
        lax.rem(lax.broadcasted_iota(jnp.int32, (24, 128), 0), 8)
        == lax.broadcasted_iota(jnp.int32, (24, 128), 1)
    ).astype(BF16)
    edges = ((0, ROWS), (ext - ROWS, ROWS))
    regions = (((ROWS, inner_rows),), edges)

    def pieces_of(region):
        count = sum(size for _, size in regions[region])
        return [(at, min(128, count - at)) for at in range(0, count, 128)]

    def rows_of(buf, region):
        got = [buf[pl.ds(first, size), :] for first, size in regions[region]]
        return got[0] if len(got) == 1 else jnp.concatenate(got, axis=0)

    def row_sums(v):
        a, b, c = (dot(ones, term, NT) for term in split3(v))
        return a + b + c

    def columns(at, region, one, two):
        line = lax.broadcasted_iota(jnp.int32, (8, one.shape[1]), 0)
        both = jnp.where(line == 0, one, jnp.where(line == 1, two, 0.0))
        terms = [term.astype(F32) for term in split3(both)]
        got = dot(jnp.concatenate(terms, axis=0).astype(BF16), eye, TN)
        done = 0
        for first, size in regions[region]:
            cols[at, pl.ds(first, size), :] = got[done : done + size]
            done += size

    def stat_copy(at, off):
        return pltpu.make_async_remote_copy(
            src_ref=stats.at[at, 0],
            dst_ref=stats.at[at, off],
            send_sem=stat_send.at[at],
            recv_sem=stat_recv.at[at],
            device_id={"dp": lax.rem(d + off, dp)},
            device_id_type=MESH,
        )

    def stat_all(at):
        every = stats.at[at, pl.ds(1, dp - 1)]
        return pltpu.make_async_remote_copy(
            src_ref=every,
            dst_ref=every,
            send_sem=stat_send.at[at],
            recv_sem=stat_recv.at[at],
            device_id={"dp": lax.rem(d + 1, dp)},
            device_id_type=MESH,
        )

    def stat_start(at, region, one, two):
        pieces = pieces_of(region)
        stats[at, 0] = jnp.zeros(stats.shape[2:], F32)
        for first, sums in ((0, row_sums(one)), (len(pieces), row_sums(two))):
            for j, (begin, size) in enumerate(pieces):
                stats[at, 0, first + j : first + j + 1, 0:size] = sums[0:1, begin : begin + size]
        for off in range(1, dp):
            stat_copy(at, off).start()

    def stat_wait(at, region):
        pieces = pieces_of(region)
        stat_all(at).wait_recv()
        total = stats[at, 0]
        for off in range(1, dp):
            total = total + stats[at, off]
        total = total * (1.0 / channels)
        return tuple(
            jnp.concatenate(
                [total[first + j : first + j + 1, 0:size] for j, (_, size) in enumerate(pieces)],
                axis=1,
            )
            for first in (0, len(pieces))
        )

    def moments_start(region):
        v = rows_of(mixed, region)
        stat_start(region, region, v, v * v)

    def moments_wait(region):
        mean, square = stat_wait(region, region)
        columns(0, region, mean, lax.rsqrt(square - mean * mean + EPS))

    def second_start(region):
        v = rows_of(d_act, region)
        stat_start(2 + region, region, v, v * rows_of(mixed, region))

    def second_wait(region):
        columns(1, region, *stat_wait(2 + region, region))

    row_loop(conv, begin=ROWS, end=ext - ROWS)
    moments_start(0)
    halo_wait(glu, 2 * PAD, 0)

    def conv_edge(i, _):
        conv(pl.multiple_of(i * (ext - ROWS), ROWS), None)

    lax.fori_loop(0, 2, conv_edge, None)
    moments_start(1)
    halo_wait(d_act, PAD, 2)

    def norm_rows(r, rows):
        here = pl.ds(r, rows)
        col = cols[0, here, :]
        centred = (mixed[here, :] - col[:, 0:1]) * col[:, 1:2]
        normed = centred * gain[...] + shift[...]
        sig = jax.nn.sigmoid(normed)
        act[here, :] = (normed * sig).astype(BF16)
        d_normed = d_act[here, :] * sig * (1.0 + normed * (1.0 - sig))
        mixed[here, :] = centred
        d_act[here, :] = d_normed * gain[...]
        return d_normed * centred, d_normed

    def down(v):
        return jnp.sum(v, axis=0, keepdims=True)

    def norm(r, carry):
        return tuple(had + down(v) for had, v in zip(carry, norm_rows(r, big)))

    zero = jnp.zeros((1, chans), F32)
    moments_wait(0)
    sums = row_loop(norm, (zero, zero), big, ROWS, ext - ROWS)
    second_start(0)
    moments_wait(1)
    kept = (slice(PAD, ROWS), slice(0, ROWS - PAD))
    for (first, size), keep in zip(edges, kept):
        sums = tuple(had + down(v[keep]) for had, v in zip(sums, norm_rows(first, size)))
    gain_sum, shift_sum = sums
    second_start(1)

    def several(count, fn):
        if count <= 8:
            for i in range(count):
                fn(i)
        else:
            lax.fori_loop(0, count, lambda i, _: fn(i), None)

    def grad_tile(at, rows, off):
        index = index_of(lax.rem(pos + off + 2 * sp, sp))
        those = pl.ds(pl.multiple_of(index * chunk, chunk), chunk)
        part[at, pl.ds(pl.multiple_of(index * lines, lines), lines), :] = dot(
            turned[at], rows[:, those], NN
        )

    def grad_first(at, rows, factor):
        if wide:
            turned[at] = factor.T
            grad_tile(at, rows, -1)
            grad_tile(at, rows, 1)
            return

        def step(i, _):
            here = pl.ds(pl.multiple_of(i * tile, tile), tile)
            part[at, here, :] = dot(rows[:, here], factor, TN)

        lax.fori_loop(0, width // tile, step, None)

    def grad_rest(at, rows):
        if wide:
            several(sp - 2, lambda i: grad_tile(at, rows, (i + 2) % (sp - 1)))

    streams = [
        (at, 2 * sub + (way < 0), way) for at in range(3) for sub in range(SUBS) for way in (1, -1)
    ]
    early = [i for i, (at, _, _) in enumerate(streams) if at == 2]
    late = [i for sub in range(SUBS) for i, (at, place, _) in enumerate(streams) if at < 2 and place // 2 == sub]

    def late_of(at):
        return [i for i in late if streams[i][0] == at]

    def piece(stream, p):
        at, place, _ = streams[stream]
        first = index_of(lax.rem(p + 2 * sp, sp)) * lines + place * strip
        return part[at, pl.ds(pl.multiple_of(first, strip), strip), :]

    def ring_copy(stream, k):
        return pltpu.make_async_remote_copy(
            src_ref=ring_src.at[stream, k],
            dst_ref=ring_dst.at[stream, k],
            send_sem=ring_send.at[0],
            recv_sem=ring_recv.at[stream, k],
            device_id={"sp": ahead if streams[stream][2] == 1 else behind},
            device_id_type=MESH,
        )

    def ring_step(k, which):
        for stream in which:
            way = streams[stream][2]
            mine = piece(stream, pos - way * (1 + k))
            if not (isinstance(k, int) and k == 0):
                ring_copy(stream, k - 1).wait_recv()
                mine = mine + ring_dst[stream, k - 1].astype(F32)
            ring_src[stream, k] = mine.astype(BF16)
            ring_copy(stream, k).start()

    def ring_end(which, outs):
        for stream in which:
            at, place, _ = streams[stream]
            ring_copy(stream, sp - 2).wait_recv()
            outs[at][pl.ds(place * strip, strip), :] = ratio * (
                piece(stream, pos) + ring_dst[stream, sp - 2].astype(F32)
            )

    grad_first(2, og, act[own, :])
    ring_step(0, early)
    grad_rest(2, og)

    def back_rows(r, rows):
        here = pl.ds(r, rows)
        col, back = cols[0, here, :], cols[1, here, :]
        d_mixed = col[:, 1:2] * (d_act[here, :] - back[:, 0:1] - mixed[here, :] * back[:, 1:2])
        d_pad[here, :] = d_mixed
        return d_mixed

    def norm_back(r, bias_sum):
        return bias_sum + down(back_rows(r, big))

    second_wait(0)
    bias_sum = row_loop(norm_back, zero, big, ROWS, ext - ROWS)
    second_wait(1)
    for (first, size), keep in zip(edges, kept):
        bias_sum = bias_sum + down(back_rows(first, size)[keep])
    halo_zero(d_pad, PAD)

    def conv_back(r, _):
        here = pl.ds(r, ROWS)
        acc = jnp.zeros((ROWS, chans), F32)
        acc = slide(d_pad, r, lambda tap: PAD + reach - tap, acc)
        o = opening[here, :]
        grad = acc * o
        dv[here, :] = grad.astype(BF16)
        dg[here, :] = (grad * value[here, :] * (1.0 - o)).astype(BF16)

    middle = tokens // ROWS // 2 * ROWS
    row_loop(conv_back, end=middle)
    ring_step(1, early)
    row_loop(conv_back, begin=middle)
    grad_first(0, x, dv[...])
    ring_step(0, late_of(0))
    grad_first(1, x, dg[...])
    ring_step(0, late_of(1))
    grad_rest(0, x)
    grad_rest(1, x)
    ring_step(2, early)

    half = tokens // 2
    mine = pl.multiple_of(lax.rem(d, 2) * half, half)
    other = pl.multiple_of((1 - lax.rem(d, 2)) * half, half)
    group = width // GROUPS

    def ig_copy(at, g, src, dst, bit):
        return pltpu.make_async_remote_copy(
            src_ref=src,
            dst_ref=dst,
            send_sem=ig_ssem.at[at],
            recv_sem=give_rsem.at[0] if at == bits_dp else ig_rsem.at[at, g],
            device_id={"dp": flip(d, bit)},
            device_id_type=MESH,
        )

    def of_group(g):
        return pl.ds(g * group, group)

    def pair_copy(g):
        return ig_copy(0, g, ig_send.at[:, of_group(g)], ig_recv.at[:, of_group(g)], 0)

    def y_copy(bit, g):
        return ig_copy(
            bit, g, ig_sum.at[bit - 1, :, of_group(g)], ig_peer.at[bit - 1, :, of_group(g)], bit
        )

    final = bits_dp - 1

    def give_copy(g):
        return ig_copy(
            bits_dp,
            g,
            ig_sum.at[final, :, of_group(g)],
            ig_out.at[pl.ds(mine, half), of_group(g)],
            0,
        )

    both_v = jnp.concatenate([dv[pl.ds(other, half), :], dv[pl.ds(mine, half), :]], axis=0)
    both_g = jnp.concatenate([dg[pl.ds(other, half), :], dg[pl.ds(mine, half), :]], axis=0)
    size = min(tile, group)
    for g in range(GROUPS):
        for begin in range(g * group, (g + 1) * group, size):
            here = pl.ds(begin, size)
            got = dot(both_v, wv[here, :], NT) + dot(both_g, wg[here, :], NT)
            ig_send[:, here] = got[:half].astype(BF16)
            ig_own[:, here] = got[half:]
        pair_copy(g).start()

    def pair_sums():
        for g in range(GROUPS):
            pair_copy(g).wait_recv()
            here = of_group(g)
            ig_sum[0, :, here] = (ig_own[:, here] + ig_recv[:, here].astype(F32)).astype(BF16)
            if bits_dp > 1:
                y_copy(1, g).start()

    small[0] = jnp.zeros(small.shape[1:], F32)

    def taps_grad(low):
        those = [
            [tap for tap in range(taps) if (tap + PAD - reach) % 8 == low + at] for at in range(2)
        ]

        def taps_sum(r, sums):
            grad = d_pad[pl.ds(r + PAD, ROWS), :]
            new = []
            for at in range(2):
                window = shifted(glu, r + PAD, low + at)
                for tap in those[at]:
                    high = tap + PAD - reach - low - at
                    prod = grad * window[high : high + ROWS]
                    acc = sums[len(new)]
                    for row in range(0, ROWS, 8):
                        acc = acc + prod[row : row + 8]
                    new.append(acc)
            return tuple(new)

        flat = those[0] + those[1]
        sums = row_loop(taps_sum, tuple(jnp.zeros((8, chans), F32) for _ in flat))
        for acc, tap in zip(sums, flat):
            small[0, tap : tap + 1, :] = jnp.sum(acc, axis=0, keepdims=True) * ratio

    def small_copy(bit):
        return pltpu.make_async_remote_copy(
            src_ref=small.at[bit],
            dst_ref=small_recv.at[bit],
            send_sem=small_ssem.at[0],
            recv_sem=small_rsem.at[bit],
            device_id={"sp": flip(s, bit)},
            device_id_type=MESH,
        )

    def small_first():
        small[0, taps : taps + 1, :] = bias_sum * ratio
        small[0, taps + 1 : taps + 2, :] = gain_sum * ratio
        small[0, taps + 2 : taps + 3, :] = shift_sum * ratio
        small_copy(0).start()

    def small_next(bit):
        if bit < bits_sp:
            small_copy(bit).wait_recv()
            small[bit + 1] = small[bit] + small_recv[bit]
            if bit + 1 < bits_sp:
                small_copy(bit + 1).start()

    def taps_half(lows):
        for low in lows:
            taps_grad(low)

    pair_sums()
    fixed = min(sp - 2, 6)
    for k in range(1, fixed + 1):
        ring_step(k, late)
        if k + 2 <= sp - 2:
            ring_step(k + 2, early)
        if k == 1:
            taps_half((0, 2))
        if k == 2:
            taps_half((4, 6))
            small_first()
        if k > 2:
            small_next(k - 3)
    for bit in range(max(fixed - 2, 0), bits_sp):
        small_next(bit)
    if sp - 2 > fixed:

        def both(k, _):
            ring_step(k, late)
            ring_step(k + 2, early)

        lax.fori_loop(fixed + 1, sp - 3, both, None)
        ring_step(sp - 3, late)
        ring_step(sp - 2, late)

    for bit in range(1, bits_dp):
        for g in range(GROUPS):
            y_copy(bit, g).wait_recv()
            here = of_group(g)
            got = ig_sum[bit - 1, :, here].astype(F32) + ig_peer[bit - 1, :, here].astype(F32)
            ig_sum[bit, :, here] = got.astype(BF16)
            if bit + 1 < bits_dp:
                y_copy(bit + 1, g).start()
            else:
                give_copy(g).start()
    if bits_dp == 1:
        for g in range(GROUPS):
            give_copy(g).start()
    ig_out[pl.ds(mine, half), :] = ig_sum[final]
    small_out[...] = small[bits_sp]
    ring_end(early + late, (vg_out, gg_out, dg_out))

    ig_copy(0, 0, ig_send, ig_recv, 0).wait_send()
    for bit in range(1, bits_dp):
        ig_copy(bit, 0, ig_sum.at[bit - 1], ig_peer.at[bit - 1], bit).wait_send()
    ig_copy(bits_dp, 0, ig_sum.at[final], ig_out.at[pl.ds(mine, half)], 0).wait()
    for at in range(4):
        stat_all(at).wait_send()
    rounds = small.at[pl.ds(0, bits_sp)]
    pltpu.make_async_remote_copy(
        src_ref=rounds,
        dst_ref=rounds,
        send_sem=small_ssem.at[0],
        recv_sem=small_rsem.at[0],
        device_id={"sp": flip(s, 0)},
        device_id_type=MESH,
    ).wait_send()
    pltpu.make_async_remote_copy(
        src_ref=ring_src,
        dst_ref=ring_dst,
        send_sem=ring_send.at[0],
        recv_sem=ring_recv.at[0, 0],
        device_id={"sp": ahead},
        device_id_type=MESH,
    ).wait_send()


def finish(
    wide, ig, vg, gg, dgrad, small, ig_o, vg_o, gg_o, dg_o, k_o, b_o, g_o, s_o,
    t0, t1, k_v, b_v, g_v, s_v, sem,
):
    copies = []

    def send(src, dst):
        copies.append(pltpu.make_async_copy(src, dst, sem.at[len(copies)]))
        copies[-1].start()

    send(ig, ig_o)
    turn = [(vg, vg_o), (gg, gg_o)] if wide else [(dgrad, dg_o)]
    keep = [(dgrad, dg_o)] if wide else [(vg, vg_o), (gg, gg_o)]
    for src, dst in keep:
        send(src, dst)
    taps = k_o.shape[0]
    k_v[...] = small[0:taps, :]
    send(k_v, k_o)
    for at, (held, out) in enumerate(((b_v, b_o), (g_v, g_o), (s_v, s_o))):
        held[...] = small[taps + at, :]
        send(held, out)
    for (src, dst), held in zip(turn, (t0, t1)):
        held[...] = src[...].T
        send(held, dst)
    for copy in copies:
        copy.wait()


def on_device(
    normed_input,
    out_grad,
    value_weight,
    gate_weight,
    down_weight,
    conv_kernel,
    conv_bias,
    norm_gain,
    norm_shift,
):
    tokens, width = normed_input.shape
    taps, chans = conv_kernel.shape
    sp, dp = lax.axis_size("sp"), lax.axis_size("dp")
    ratio = 1.0 / math.sqrt(tokens * sp)
    chunk = width // sp
    bits_sp, bits_dp = sp.bit_length() - 1, dp.bit_length() - 1
    small_rows = -(-(taps + 3) // 8) * 8
    half = tokens // 2
    full, extended = (tokens, chans), (tokens + 2 * PAD, chans)
    vmem = pl.BlockSpec(memory_space=pltpu.VMEM)
    hbm = pl.BlockSpec(memory_space=pltpu.HBM)
    dma = pltpu.SemaphoreType.DMA
    wide = is_wide(chunk, chans)
    lines, lanes = (chans, chunk) if wide else (chunk, chans)
    stat_rows = -(-2 * -(-tokens // 128) // 8) * 8
    count = 3 * 2 * SUBS
    ig, vg, gg, dgrad, small = pl.pallas_call(
        functools.partial(kernel, sp, dp, ratio),
        out_shape=(
            pltpu.VMEM((tokens, width), BF16),
            pltpu.VMEM((lines, lanes), F32),
            pltpu.VMEM((lines, lanes), F32),
            pltpu.VMEM((lines, lanes), F32),
            pltpu.VMEM((small_rows, chans), F32),
        ),
        in_specs=[hbm] * 9,
        out_specs=(vmem,) * 5,
        scratch_shapes=[
            pltpu.VMEM((tokens, width), BF16),
            pltpu.VMEM((tokens, width), BF16),
            pltpu.VMEM((width, chans), BF16),
            pltpu.VMEM((width, chans), BF16),
            pltpu.VMEM((chans, width), BF16),
            pltpu.VMEM((taps, chans), F32),
            pltpu.VMEM((1, chans), F32),
            pltpu.VMEM((1, chans), F32),
            pltpu.VMEM((1, chans), F32),
            dma((9,)),
            pltpu.VMEM(full, F32),
            pltpu.VMEM(full, F32),
            pltpu.VMEM((tokens + 4 * PAD, chans), F32),
            pltpu.VMEM(extended, F32),
            pltpu.VMEM(extended, F32),
            pltpu.VMEM(extended, F32),
            pltpu.VMEM(extended, BF16),
            pltpu.VMEM(full, BF16),
            pltpu.VMEM(full, BF16),
            pltpu.VMEM((3, chans, tokens), BF16),
            pltpu.VMEM((2, tokens + 2 * PAD, 128), F32),
            pltpu.VMEM((4, dp, stat_rows, 128), F32),
            pltpu.VMEM((3, sp * lines, lanes), F32),
            pltpu.VMEM((count, sp - 1, lines // (2 * SUBS), lanes), BF16),
            pltpu.VMEM((count, sp - 1, lines // (2 * SUBS), lanes), BF16),
            pltpu.VMEM((half, width), BF16),
            pltpu.VMEM((half, width), BF16),
            pltpu.VMEM((half, width), F32),
            pltpu.VMEM((bits_dp, half, width), BF16),
            pltpu.VMEM((bits_dp - 1, half, width), BF16),
            pltpu.VMEM((bits_sp + 1, small_rows, chans), F32),
            pltpu.VMEM((bits_sp, small_rows, chans), F32),
            dma((4,)),
            dma((4,)),
            dma((4,)),
            dma((4,)),
            dma((1,)),
            dma((count, sp - 1)),
            dma((bits_dp + 1,)),
            dma((bits_dp, GROUPS)),
            dma((1,)),
            dma((1,)),
            dma((bits_sp,)),
        ],
        compiler_params=pltpu.CompilerParams(
            collective_id=0, has_side_effects=True, vmem_limit_bytes=MAIN
        ),
    )(
        normed_input,
        out_grad,
        value_weight,
        gate_weight,
        down_weight,
        conv_kernel,
        conv_bias[None, :],
        norm_gain[None, :],
        norm_shift[None, :],
    )
    row = jax.ShapeDtypeStruct((chans,), F32)
    return pl.pallas_call(
        functools.partial(finish, wide),
        out_shape=(
            jax.ShapeDtypeStruct(ig.shape, BF16),
            jax.ShapeDtypeStruct(vg.shape, F32),
            jax.ShapeDtypeStruct(gg.shape, F32),
            jax.ShapeDtypeStruct((chans, chunk), F32),
            jax.ShapeDtypeStruct((taps, chans), F32),
            row,
            row,
            row,
        ),
        in_specs=[vmem] * 5,
        out_specs=(hbm,) * 8,
        scratch_shapes=[
            pltpu.VMEM((lanes, lines), F32),
            pltpu.VMEM((lanes, lines), F32),
            pltpu.VMEM((taps, chans), F32),
            pltpu.VMEM((chans,), F32),
            pltpu.VMEM((chans,), F32),
            pltpu.VMEM((chans,), F32),
            dma((8,)),
        ],
        compiler_params=pltpu.CompilerParams(vmem_limit_bytes=FINISH),
    )(ig, vg, gg, dgrad, small)


def solution(mesh):
    in_specs = (
        P("sp", None),
        P("sp", None),
        P(None, "dp"),
        P(None, "dp"),
        P("dp", None),
        P(None, "dp"),
        P("dp"),
        P("dp"),
        P("dp"),
    )
    out_specs = (
        P("sp", None),
        P("sp", "dp"),
        P("sp", "dp"),
        P("dp", "sp"),
        P(None, "dp"),
        P("dp"),
        P("dp"),
        P("dp"),
    )
    return jax.shard_map(
        on_device, mesh=mesh, in_specs=in_specs, out_specs=out_specs, check_vma=False
    )
```

```python
import functools
import math

import jax
import jax.numpy as jnp
from jax import lax
from jax.experimental import pallas as pl
from jax.experimental.pallas import tpu as pltpu
from jax.sharding import PartitionSpec as P

EPS = 1e-05
F32 = jnp.float32
BF16 = jnp.bfloat16
MESH = pl.DeviceIdType.MESH
NN = (((1,), (0,)), ((), ()))
NT = (((1,), (1,)), ((), ()))
TN = (((0,), (0,)), ((), ()))
PAD = 16
ROWS = 32
SUBS = 2
GROUPS = 2
MAIN = 61_900_000
FINISH = 16_000_000


def dot(a, b, numbers):
    return lax.dot_general(a, b, numbers, preferred_element_type=F32)


def split3(v):
    high = v.astype(BF16)
    rest = v - high.astype(F32)
    mid = rest.astype(BF16)
    return high, mid, (rest - mid.astype(F32)).astype(BF16)


def is_wide(chunk, chans):
    return chunk % 128 == 0 and chans % 32 == 0


def is_paired(sp, dp, chunk, chans):
    return is_wide(chunk, chans) and chans % 256 == 0 and sp % 4 == 0 and sp >= 8 and dp % 2 == 0


def kernel(
    sp,
    dp,
    ratio,
    x_hbm,
    og_hbm,
    wv_hbm,
    wg_hbm,
    wd_hbm,
    ck_hbm,
    bias_hbm,
    gain_hbm,
    shift_hbm,
    ig_out,
    vg_out,
    gg_out,
    dg_out,
    small_out,
    x,
    og,
    wv,
    wg,
    wd,
    ck,
    bias,
    gain,
    shift,
    load_sem,
    value,
    opening,
    glu,
    mixed,
    d_act,
    d_pad,
    act,
    dv,
    dg,
    turned,
    cols,
    stats,
    part,
    ring_src,
    ring_dst,
    ig_send,
    ig_recv,
    ig_own,
    ig_sum,
    ig_peer,
    small,
    small_recv,
    halo_send,
    halo_recv,
    stat_send,
    stat_recv,
    ring_send,
    ring_recv,
    ig_ssem,
    ig_rsem,
    give_rsem,
    small_ssem,
    small_rsem,
    xp,
    ogp,
    in_recv,
    lhs,
    x_send,
    x_recv,
    held,
    z_send,
    z_recv,
    pair_sends,
    near_recv,
    in_rsem,
    x_rsem,
    z_rsem,
):
    tokens, width = x.shape
    taps, chans = ck.shape
    channels = chans * dp
    reach = taps // 2
    chunk = width // sp
    wide = is_wide(chunk, chans)
    paired = is_paired(sp, dp, chunk, chans)
    lines = chans if wide else chunk
    strip = lines // (2 * SUBS)
    tile = min(256, width)
    s = lax.axis_index("sp")
    d = lax.axis_index("dp")
    bits_sp = sp.bit_length() - 1
    bits_dp = dp.bit_length() - 1

    def flip(i, bit):
        step = 1 << bit
        return i + step * (1 - 2 * lax.rem(lax.div(i, step), 2))

    def index_of(p):
        far = lax.div(p, sp // 2)
        return (1 - far) * 2 * p + far * (2 * sp - 1 - 2 * p)

    odd = lax.rem(s, 2)
    pos = (1 - odd) * lax.div(s, 2) + odd * (sp - 1 - lax.div(s, 2))
    ahead = index_of(lax.rem(pos + 1, sp))
    behind = index_of(lax.rem(pos + sp - 1, sp))

    loads = [
        pltpu.make_async_copy(src, dst, load_sem.at[at])
        for at, (src, dst) in enumerate(
            [
                (x_hbm, x),
                (wv_hbm, wv),
                (wg_hbm, wg),
                (og_hbm, og),
                (wd_hbm, wd),
                (ck_hbm, ck),
                (bias_hbm, bias),
                (gain_hbm, gain),
                (shift_hbm, shift),
            ]
        )
    ]
    for load in loads:
        load.start()

    barrier = pltpu.get_barrier_semaphore()
    peers = [ahead, behind, lax.rem(s + 1, sp), lax.rem(s + sp - 1, sp)]
    peers += [flip(s, bit) for bit in range(bits_sp)]
    quads = sp // 4
    if paired and quads > 2:
        peers += [lax.rem(s + 4 * far, sp) for far in range(1, quads)]
    for peer in peers:
        pl.semaphore_signal(barrier, inc=1, device_id={"sp": peer}, device_id_type=MESH)
    for off in range(1, dp):
        pl.semaphore_signal(
            barrier, inc=1, device_id={"dp": lax.rem(d + off, dp)}, device_id_type=MESH
        )

    for load in loads[:3]:
        load.wait()
    value_f, gate_f = dot(x[...], wv[...], NN), dot(x[...], wg[...], NN)
    value[...] = value_f.astype(BF16).astype(F32)
    opening[...] = gate_f.astype(BF16).astype(F32)

    def row_loop(fn, init=None, rows=ROWS, begin=0, end=tokens):
        def step(i, carry):
            return fn(pl.multiple_of(begin + i * rows, math.gcd(begin, rows)), carry)

        return lax.fori_loop(0, (end - begin) // rows, step, init)

    ext = tokens + 2 * PAD
    inner_rows = ext - 2 * ROWS
    big = 96 if inner_rows % 96 == 0 else ROWS
    own = pl.ds(PAD, tokens)

    def make_glu(r, _):
        here = pl.ds(r, ROWS)
        o = jax.nn.sigmoid(opening[here, :])
        opening[here, :] = o
        glu[pl.ds(r + 2 * PAD, ROWS), :] = value[here, :] * o

    row_loop(make_glu)
    pl.semaphore_wait(barrier, len(peers) + dp - 1)

    has_low, has_high = s > 0, s < sp - 1

    def halo_copies(buf, pad, at):
        up = pltpu.make_async_remote_copy(
            src_ref=buf.at[pl.ds(tokens, pad)],
            dst_ref=buf.at[pl.ds(0, pad)],
            send_sem=halo_send.at[at],
            recv_sem=halo_recv.at[at],
            device_id={"sp": lax.rem(s + 1, sp)},
            device_id_type=MESH,
        )
        down = pltpu.make_async_remote_copy(
            src_ref=buf.at[pl.ds(pad, pad)],
            dst_ref=buf.at[pl.ds(tokens + pad, pad)],
            send_sem=halo_send.at[at + 1],
            recv_sem=halo_recv.at[at + 1],
            device_id={"sp": lax.rem(s + sp - 1, sp)},
            device_id_type=MESH,
        )
        return up, down

    def halo_zero(buf, pad):
        @pl.when(s == 0)
        def _():
            buf[pl.ds(0, pad), :] = jnp.zeros((pad, chans), F32)

        @pl.when(s == sp - 1)
        def _():
            buf[pl.ds(tokens + pad, pad), :] = jnp.zeros((pad, chans), F32)

    def halo_start(buf, pad, at):
        up, down = halo_copies(buf, pad, at)
        pl.when(has_high)(up.start)
        pl.when(has_low)(down.start)
        halo_zero(buf, pad)

    def halo_wait(buf, pad, at):
        up, down = halo_copies(buf, pad, at)

        @pl.when(has_low)
        def _():
            up.wait_recv()
            down.wait_send()

        @pl.when(has_high)
        def _():
            down.wait_recv()
            up.wait_send()

    half = tokens // 2
    hand = chans // 2
    core = lax.rem(d, 2)
    these = pl.ds(pl.multiple_of(core * half, half), half)
    slots = [(far, other) for other in (1, 0) for far in range(quads)]
    held_rows, near_rows = (x, og), (xp, ogp)
    in_bits, mid_bits = (1, 0), (0, 1)

    def columns_of(who, far, other, kind):
        index = lax.rem(who + 4 * far, sp)
        if other:
            index = flip(index, mid_bits[kind])
        return pl.ds(pl.multiple_of(index * chunk, chunk), chunk)

    def slot_of(far, other):
        return pl.ds((2 * far + other) * chunk, chunk)

    def send_to(at, src, dst, recv_sem, where):
        return pltpu.make_async_remote_copy(
            src_ref=src,
            dst_ref=dst,
            send_sem=pair_sends.at[at],
            recv_sem=recv_sem,
            device_id=where,
            device_id_type=MESH,
        )

    def near_start(kind, those):
        there = flip(s, in_bits[kind])
        for far, other in those if paired else ():
            send_to(
                kind,
                held_rows[kind].at[these, columns_of(there, far, other, kind)],
                near_rows[kind].at[these, slot_of(far, other)],
                near_recv.at[kind],
                {"sp": there},
            ).start()

    def near_all(kind, stage):
        where = {"dp": flip(d, 0)} if stage else {"sp": flip(s, in_bits[kind])}
        rows = near_rows[kind].at[these]
        at = kind + 2 * stage
        return send_to(at, rows, rows, near_recv.at[at], where)

    halo_start(glu, 2 * PAD, 0)
    near_start(0, slots[:1])
    for load in loads[3:]:
        load.wait()
    near_start(1, slots[:1])
    d_act[own, :] = dot(og[...], wd[...], NT)
    halo_start(d_act, PAD, 2)
    near_start(1, slots[1:])
    near_start(0, slots[1:])

    span = ROWS + 2 * PAD

    def shifted(buf, r, offset):
        window = buf[pl.ds(r, span), :]
        return pltpu.roll(window, span - offset, 0) if offset else window

    def slide(buf, r, offset_of, acc):
        for low in range(8):
            those = [tap for tap in range(taps) if offset_of(tap) % 8 == low]
            if those:
                window = shifted(buf, r, low)
                for tap in those:
                    high = offset_of(tap) - low
                    acc = acc + ck[tap : tap + 1, :] * window[high : high + ROWS]
        return acc

    def conv(r, _):
        acc = jnp.zeros((ROWS, chans), F32) + bias[...]
        mixed[pl.ds(r, ROWS), :] = slide(glu, r, lambda tap: tap + PAD - reach, acc)

    ones = jnp.ones((16, chans), BF16)
    eye = (
        lax.rem(lax.broadcasted_iota(jnp.int32, (24, 128), 0), 8)
        == lax.broadcasted_iota(jnp.int32, (24, 128), 1)
    ).astype(BF16)
    edges = ((0, ROWS), (ext - ROWS, ROWS))
    regions = (((ROWS, inner_rows),), edges)

    def pieces_of(region):
        count = sum(size for _, size in regions[region])
        return [(at, min(128, count - at)) for at in range(0, count, 128)]

    def rows_of(buf, region):
        got = [buf[pl.ds(first, size), :] for first, size in regions[region]]
        return got[0] if len(got) == 1 else jnp.concatenate(got, axis=0)

    def row_sums(v):
        a, b, c = (dot(ones, term, NT) for term in split3(v))
        return a + b + c

    def columns(at, region, one, two):
        line = lax.broadcasted_iota(jnp.int32, (8, one.shape[1]), 0)
        both = jnp.where(line == 0, one, jnp.where(line == 1, two, 0.0))
        terms = [term.astype(F32) for term in split3(both)]
        got = dot(jnp.concatenate(terms, axis=0).astype(BF16), eye, TN)
        done = 0
        for first, size in regions[region]:
            cols[at, pl.ds(first, size), :] = got[done : done + size]
            done += size

    def stat_copy(at, off):
        return pltpu.make_async_remote_copy(
            src_ref=stats.at[at, 0],
            dst_ref=stats.at[at, off],
            send_sem=stat_send.at[at],
            recv_sem=stat_recv.at[at],
            device_id={"dp": lax.rem(d + off, dp)},
            device_id_type=MESH,
        )

    def stat_all(at):
        every = stats.at[at, pl.ds(1, dp - 1)]
        return pltpu.make_async_remote_copy(
            src_ref=every,
            dst_ref=every,
            send_sem=stat_send.at[at],
            recv_sem=stat_recv.at[at],
            device_id={"dp": lax.rem(d + 1, dp)},
            device_id_type=MESH,
        )

    def stat_start(at, region, one, two):
        pieces = pieces_of(region)
        stats[at, 0] = jnp.zeros(stats.shape[2:], F32)
        for first, sums in ((0, row_sums(one)), (len(pieces), row_sums(two))):
            for j, (begin, size) in enumerate(pieces):
                stats[at, 0, first + j : first + j + 1, 0:size] = sums[0:1, begin : begin + size]
        for off in range(1, dp):
            stat_copy(at, off).start()

    def stat_wait(at, region):
        pieces = pieces_of(region)
        stat_all(at).wait_recv()
        total = stats[at, 0]
        for off in range(1, dp):
            total = total + stats[at, off]
        total = total * (1.0 / channels)
        return tuple(
            jnp.concatenate(
                [total[first + j : first + j + 1, 0:size] for j, (_, size) in enumerate(pieces)],
                axis=1,
            )
            for first in (0, len(pieces))
        )

    def moments_start(region):
        v = rows_of(mixed, region)
        stat_start(region, region, v, v * v)

    def moments_wait(region):
        mean, square = stat_wait(region, region)
        columns(0, region, mean, lax.rsqrt(square - mean * mean + EPS))

    def second_start(region):
        v = rows_of(d_act, region)
        stat_start(2 + region, region, v, v * rows_of(mixed, region))

    def second_wait(region):
        columns(1, region, *stat_wait(2 + region, region))

    row_loop(conv, begin=ROWS, end=ext - ROWS)
    moments_start(0)
    halo_wait(glu, 2 * PAD, 0)

    def conv_edge(i, _):
        conv(pl.multiple_of(i * (ext - ROWS), ROWS), None)

    lax.fori_loop(0, 2, conv_edge, None)
    moments_start(1)

    def norm_rows(r, rows):
        here = pl.ds(r, rows)
        col = cols[0, here, :]
        centred = (mixed[here, :] - col[:, 0:1]) * col[:, 1:2]
        normed = centred * gain[...] + shift[...]
        sig = jax.nn.sigmoid(normed)
        act[here, :] = (normed * sig).astype(BF16)
        d_normed = d_act[here, :] * sig * (1.0 + normed * (1.0 - sig))
        mixed[here, :] = centred
        d_act[here, :] = d_normed * gain[...]
        return d_normed * centred, d_normed

    def down(v):
        return jnp.sum(v, axis=0, keepdims=True)

    def norm(r, carry):
        return tuple(had + down(v) for had, v in zip(carry, norm_rows(r, big)))

    zero = jnp.zeros((1, chans), F32)
    moments_wait(0)
    sums = row_loop(norm, (zero, zero), big, ROWS, ext - ROWS)
    second_start(0)
    halo_wait(d_act, PAD, 2)
    moments_wait(1)
    kept = (slice(PAD, ROWS), slice(0, ROWS - PAD))
    for (first, size), keep in zip(edges, kept):
        sums = tuple(had + down(v[keep]) for had, v in zip(sums, norm_rows(first, size)))
    gain_sum, shift_sum = sums
    second_start(1)

    def several(count, fn):
        if count <= 8:
            for i in range(count):
                fn(i)
        else:
            lax.fori_loop(0, count, lambda i, _: fn(i), None)

    def grad_tile(at, rows, off):
        index = index_of(lax.rem(pos + off + 2 * sp, sp))
        those = pl.ds(pl.multiple_of(index * chunk, chunk), chunk)
        part[at, pl.ds(pl.multiple_of(index * lines, lines), lines), :] = dot(
            turned[at], rows[:, those], NN
        )

    def grad_first(at, rows, factor):
        if wide:
            turned[at] = factor.T
            grad_tile(at, rows, -1)
            grad_tile(at, rows, 1)
            return

        def step(i, _):
            here = pl.ds(pl.multiple_of(i * tile, tile), tile)
            part[at, here, :] = dot(rows[:, here], factor, TN)

        lax.fori_loop(0, width // tile, step, None)

    def grad_rest(at, rows):
        if wide:
            several(sp - 2, lambda i: grad_tile(at, rows, (i + 2) % (sp - 1)))

    streams = [
        (at, 2 * sub + (way < 0), way) for at in range(3) for sub in range(SUBS) for way in (1, -1)
    ]
    early = [i for i, (at, _, _) in enumerate(streams) if at == 2]
    late = [i for sub in range(SUBS) for i, (at, place, _) in enumerate(streams) if at < 2 and place // 2 == sub]

    def late_of(at):
        return [i for i in late if streams[i][0] == at]

    def piece(stream, p):
        at, place, _ = streams[stream]
        first = index_of(lax.rem(p + 2 * sp, sp)) * lines + place * strip
        return part[at, pl.ds(pl.multiple_of(first, strip), strip), :]

    def ring_copy(stream, k):
        return pltpu.make_async_remote_copy(
            src_ref=ring_src.at[stream, k],
            dst_ref=ring_dst.at[stream, k],
            send_sem=ring_send.at[0],
            recv_sem=ring_recv.at[stream, k],
            device_id={"sp": ahead if streams[stream][2] == 1 else behind},
            device_id_type=MESH,
        )

    def ring_step(k, which):
        for stream in which:
            way = streams[stream][2]
            mine = piece(stream, pos - way * (1 + k))
            if not (isinstance(k, int) and k == 0):
                ring_copy(stream, k - 1).wait_recv()
                mine = mine + ring_dst[stream, k - 1].astype(F32)
            ring_src[stream, k] = mine.astype(BF16)
            ring_copy(stream, k).start()

    def ring_end(which, outs):
        for stream in which:
            at, place, _ = streams[stream]
            ring_copy(stream, sp - 2).wait_recv()
            outs[at][pl.ds(place * strip, strip), :] = ratio * (
                piece(stream, pos) + ring_dst[stream, sp - 2].astype(F32)
            )

    blocks = [(at, hand * place) for at in (2, 0, 1) for place in range(2)]

    def kind_of(n):
        return int(blocks[n][0] == 2)

    def factor_of(n):
        at, first = blocks[n]
        those = pl.ds(first, hand)
        return (dv, dg, act)[at].at[own if at == 2 else pl.ds(0, tokens), those]

    def in_copy(n):
        where = {"sp": flip(s, in_bits[kind_of(n)])}
        return send_to(4, factor_of(n), in_recv.at[n], in_rsem.at[n], where)

    def mid_copy(n):
        where = {"sp": flip(s, mid_bits[kind_of(n)])}
        return send_to(5, x_send.at[n], x_recv.at[n], x_rsem.at[n], where)

    def far_copy(n, far):
        where = {"sp": lax.rem(s + 4 * far, sp)}
        return send_to(
            6, z_send.at[n, far - 1], z_recv.at[n, far - 1], z_rsem.at[n, far - 1], where
        )

    def product(n):
        kind = kind_of(n)
        in_copy(n).wait_recv()
        lhs[...] = jnp.concatenate([factor_of(n)[...], in_recv[n]], axis=0).T
        for far, other in slots:
            mine = held_rows[kind][:, columns_of(s, far, other, kind)]
            rows = jnp.concatenate([mine, near_rows[kind][:, slot_of(far, other)]], axis=0)
            got = dot(lhs[...], rows, NN)
            if other:
                x_send[n, far] = got.astype(BF16)
            else:
                held[n, far] = got
            if (far, other) == (quads - 1, 1):
                mid_copy(n).start()

    def meet(n):
        mid_copy(n).wait_recv()
        for far in range(1, quads):
            z_send[n, far - 1] = (held[n, far] + x_recv[n, far].astype(F32)).astype(BF16)
            far_copy(n, far).start()
        held[n, 0] = held[n, 0] + x_recv[n, 0].astype(F32)

    def settle(n, outs):
        at, first = blocks[n]
        total = held[n, 0]
        for far in range(1, quads):
            far_copy(n, far).wait_recv()
            total = total + z_recv[n, far - 1].astype(F32)
        outs[at][pl.ds(first, hand), :] = ratio * total

    if paired:
        for n in range(2):
            in_copy(n).start()
    else:
        grad_first(2, og, act[own, :])
        ring_step(0, early)
        grad_rest(2, og)

    def back_rows(r, rows):
        here = pl.ds(r, rows)
        col, back = cols[0, here, :], cols[1, here, :]
        d_mixed = col[:, 1:2] * (d_act[here, :] - back[:, 0:1] - mixed[here, :] * back[:, 1:2])
        d_pad[here, :] = d_mixed
        return d_mixed

    def norm_back(r, bias_sum):
        return bias_sum + down(back_rows(r, big))

    second_wait(0)
    bias_sum = row_loop(norm_back, zero, big, ROWS, ext - ROWS)
    second_wait(1)
    for (first, size), keep in zip(edges, kept):
        bias_sum = bias_sum + down(back_rows(first, size)[keep])
    halo_zero(d_pad, PAD)

    def conv_back(r, _):
        here = pl.ds(r, ROWS)
        acc = jnp.zeros((ROWS, chans), F32)
        acc = slide(d_pad, r, lambda tap: PAD + reach - tap, acc)
        o = opening[here, :]
        grad = acc * o
        dv[here, :] = grad.astype(BF16)
        dg[here, :] = (grad * value[here, :] * (1.0 - o)).astype(BF16)

    middle = tokens // ROWS // 2 * ROWS
    row_loop(conv_back, end=middle)
    if not paired:
        ring_step(1, early)
    row_loop(conv_back, begin=middle)
    if paired:
        for n in (2, 3):
            in_copy(n).start()
    else:
        grad_first(0, x, dv[...])
        ring_step(0, late_of(0))
        grad_first(1, x, dg[...])
        ring_step(0, late_of(1))
        grad_rest(0, x)
        grad_rest(1, x)
        ring_step(2, early)

    mine = pl.multiple_of(lax.rem(d, 2) * half, half)
    other = pl.multiple_of((1 - lax.rem(d, 2)) * half, half)
    group = width // GROUPS

    def ig_copy(at, g, src, dst, bit):
        return pltpu.make_async_remote_copy(
            src_ref=src,
            dst_ref=dst,
            send_sem=ig_ssem.at[at],
            recv_sem=give_rsem.at[0] if at == bits_dp else ig_rsem.at[at, g],
            device_id={"dp": flip(d, bit)},
            device_id_type=MESH,
        )

    def of_group(g):
        return pl.ds(g * group, group)

    def pair_copy(g):
        return ig_copy(0, g, ig_send.at[:, of_group(g)], ig_recv.at[:, of_group(g)], 0)

    def y_copy(bit, g):
        return ig_copy(
            bit, g, ig_sum.at[bit - 1, :, of_group(g)], ig_peer.at[bit - 1, :, of_group(g)], bit
        )

    final = bits_dp - 1

    def give_copy(g):
        return ig_copy(
            bits_dp,
            g,
            ig_sum.at[final, :, of_group(g)],
            ig_out.at[pl.ds(mine, half), of_group(g)],
            0,
        )

    small[0] = jnp.zeros(small.shape[1:], F32)

    def taps_grad(low):
        those = [
            [tap for tap in range(taps) if (tap + PAD - reach) % 8 == low + at] for at in range(2)
        ]

        def taps_sum(r, sums):
            grad = d_pad[pl.ds(r + PAD, ROWS), :]
            new = []
            for at in range(2):
                window = shifted(glu, r + PAD, low + at)
                for tap in those[at]:
                    high = tap + PAD - reach - low - at
                    prod = grad * window[high : high + ROWS]
                    acc = sums[len(new)]
                    for row in range(0, ROWS, 8):
                        acc = acc + prod[row : row + 8]
                    new.append(acc)
            return tuple(new)

        flat = those[0] + those[1]
        sums = row_loop(taps_sum, tuple(jnp.zeros((8, chans), F32) for _ in flat))
        for acc, tap in zip(sums, flat):
            small[0, tap : tap + 1, :] = jnp.sum(acc, axis=0, keepdims=True) * ratio

    def small_copy(bit):
        return pltpu.make_async_remote_copy(
            src_ref=small.at[bit],
            dst_ref=small_recv.at[bit],
            send_sem=small_ssem.at[0],
            recv_sem=small_rsem.at[bit],
            device_id={"sp": flip(s, (bit + 1) % bits_sp)},
            device_id_type=MESH,
        )

    def small_first():
        small[0, taps : taps + 1, :] = bias_sum * ratio
        small[0, taps + 1 : taps + 2, :] = gain_sum * ratio
        small[0, taps + 2 : taps + 3, :] = shift_sum * ratio
        small_copy(0).start()

    def small_next(bit):
        if bit < bits_sp:
            small_copy(bit).wait_recv()
            small[bit + 1] = small[bit] + small_recv[bit]
            if bit + 1 < bits_sp:
                small_copy(bit + 1).start()

    def taps_half(lows):
        for low in lows:
            taps_grad(low)

    both_v = jnp.concatenate([dv[pl.ds(other, half), :], dv[pl.ds(mine, half), :]], axis=0)
    both_g = jnp.concatenate([dg[pl.ds(other, half), :], dg[pl.ds(mine, half), :]], axis=0)
    size = min(tile, group)
    for g in range(GROUPS):
        for begin in range(g * group, (g + 1) * group, size):
            here = pl.ds(begin, size)
            got = dot(both_v, wv[here, :], NT) + dot(both_g, wg[here, :], NT)
            ig_send[:, here] = got[:half].astype(BF16)
            ig_own[:, here] = got[half:]
        pair_copy(g).start()

    def pair_sums():
        for g in range(GROUPS):
            pair_copy(g).wait_recv()
            here = of_group(g)
            ig_sum[0, :, here] = (ig_own[:, here] + ig_recv[:, here].astype(F32)).astype(BF16)
            if bits_dp > 1:
                y_copy(1, g).start()

    if paired:
        for kind in (1, 0):
            near_all(kind, 0).wait_recv()
            near_all(kind, 1).start()
        taps_half((0, 2, 4, 6))
        small_first()
        for n in (4, 5):
            in_copy(n).start()
    pair_sums()
    fixed = min(sp - 2, 6)
    if paired:
        near_all(0, 1).wait_recv()
        product(2)
        product(3)
        small_next(0)
        near_all(1, 1).wait_recv()
        product(0)
        product(1)
        product(4)
        product(5)
        meet(2)
        small_next(1)
        meet(3)
        meet(0)
        meet(4)
        meet(1)
        meet(5)
        small_next(2)
        for bit in range(3, bits_sp):
            small_next(bit)
        fixed = 0
    for k in range(1, fixed + 1):
        ring_step(k, late)
        if k + 2 <= sp - 2:
            ring_step(k + 2, early)
        if k == 1:
            taps_half((0, 2))
        if k == 2:
            taps_half((4, 6))
            small_first()
        if k > 2:
            small_next(k - 3)
    for bit in range(max(fixed - 2, 0), bits_sp if fixed else 0):
        small_next(bit)
    if sp - 2 > fixed and fixed:

        def both(k, _):
            ring_step(k, late)
            ring_step(k + 2, early)

        lax.fori_loop(fixed + 1, sp - 3, both, None)
        ring_step(sp - 3, late)
        ring_step(sp - 2, late)

    for bit in range(1, bits_dp):
        for g in range(GROUPS):
            y_copy(bit, g).wait_recv()
            here = of_group(g)
            got = ig_sum[bit - 1, :, here].astype(F32) + ig_peer[bit - 1, :, here].astype(F32)
            ig_sum[bit, :, here] = got.astype(BF16)
            if bit + 1 < bits_dp:
                y_copy(bit + 1, g).start()
            else:
                give_copy(g).start()
    if bits_dp == 1:
        for g in range(GROUPS):
            give_copy(g).start()
    ig_out[pl.ds(mine, half), :] = ig_sum[final]
    small_out[...] = small[bits_sp]
    if paired:
        for n in (2, 3, 0, 4, 1, 5):
            settle(n, (vg_out, gg_out, dg_out))
        for kind in range(2):
            near_all(kind, 0).wait_send()
            near_all(kind, 1).wait_send()
        for at, ref in ((4, in_recv), (5, x_send), (6, z_send)):
            send_to(at, ref, ref, near_recv.at[0], {"sp": flip(s, 0)}).wait_send()
    else:
        ring_end(early + late, (vg_out, gg_out, dg_out))
        pltpu.make_async_remote_copy(
            src_ref=ring_src,
            dst_ref=ring_dst,
            send_sem=ring_send.at[0],
            recv_sem=ring_recv.at[0, 0],
            device_id={"sp": ahead},
            device_id_type=MESH,
        ).wait_send()

    ig_copy(0, 0, ig_send, ig_recv, 0).wait_send()
    for bit in range(1, bits_dp):
        ig_copy(bit, 0, ig_sum.at[bit - 1], ig_peer.at[bit - 1], bit).wait_send()
    ig_copy(bits_dp, 0, ig_sum.at[final], ig_out.at[pl.ds(mine, half)], 0).wait()
    for at in range(4):
        stat_all(at).wait_send()
    rounds = small.at[pl.ds(0, bits_sp)]
    pltpu.make_async_remote_copy(
        src_ref=rounds,
        dst_ref=rounds,
        send_sem=small_ssem.at[0],
        recv_sem=small_rsem.at[0],
        device_id={"sp": flip(s, 0)},
        device_id_type=MESH,
    ).wait_send()


def finish(
    wide, ig, vg, gg, dgrad, small, ig_o, vg_o, gg_o, dg_o, k_o, b_o, g_o, s_o,
    t0, t1, k_v, b_v, g_v, s_v, sem,
):
    copies = []

    def send(src, dst):
        copies.append(pltpu.make_async_copy(src, dst, sem.at[len(copies)]))
        copies[-1].start()

    send(ig, ig_o)
    turn = [(vg, vg_o), (gg, gg_o)] if wide else [(dgrad, dg_o)]
    keep = [(dgrad, dg_o)] if wide else [(vg, vg_o), (gg, gg_o)]
    for src, dst in keep:
        send(src, dst)
    taps = k_o.shape[0]
    k_v[...] = small[0:taps, :]
    send(k_v, k_o)
    for at, (held, out) in enumerate(((b_v, b_o), (g_v, g_o), (s_v, s_o))):
        held[...] = small[taps + at, :]
        send(held, out)
    for (src, dst), held in zip(turn, (t0, t1)):
        held[...] = src[...].T
        send(held, dst)
    for copy in copies:
        copy.wait()


def on_device(
    normed_input,
    out_grad,
    value_weight,
    gate_weight,
    down_weight,
    conv_kernel,
    conv_bias,
    norm_gain,
    norm_shift,
):
    tokens, width = normed_input.shape
    taps, chans = conv_kernel.shape
    sp, dp = lax.axis_size("sp"), lax.axis_size("dp")
    ratio = 1.0 / math.sqrt(tokens * sp)
    chunk = width // sp
    bits_sp, bits_dp = sp.bit_length() - 1, dp.bit_length() - 1
    small_rows = -(-(taps + 3) // 8) * 8
    half = tokens // 2
    full, extended = (tokens, chans), (tokens + 2 * PAD, chans)
    vmem = pl.BlockSpec(memory_space=pltpu.VMEM)
    hbm = pl.BlockSpec(memory_space=pltpu.HBM)
    dma = pltpu.SemaphoreType.DMA
    wide = is_wide(chunk, chans)
    lines, lanes = (chans, chunk) if wide else (chunk, chans)
    stat_rows = -(-2 * -(-tokens // 128) // 8) * 8
    paired = is_paired(sp, dp, chunk, chans)
    if paired:
        ring_shape, ring_sems, part_shape, turned_shape = (1, 1, 16, 128), (1, 1), (1, 8, 128), (1, 16, 128)
    else:
        count = 3 * 2 * SUBS
        ring_shape, ring_sems = (count, sp - 1, lines // (2 * SUBS), lanes), (count, sp - 1)
        part_shape, turned_shape = (3, sp * lines, lanes), (3, chans, tokens)
    quads, hand = (sp // 4, chans // 2) if paired else (2, 16)
    near, wide_chunk = (tokens, chunk) if paired else (16, 128)
    pair_scratch = [
        pltpu.VMEM((near, 2 * quads * wide_chunk), BF16),
        pltpu.VMEM((near, 2 * quads * wide_chunk), BF16),
        pltpu.VMEM((6, near, hand), BF16),
        pltpu.VMEM((hand, 2 * near), BF16),
        pltpu.VMEM((6, quads, hand, wide_chunk), BF16),
        pltpu.VMEM((6, quads, hand, wide_chunk), BF16),
        pltpu.VMEM((6, quads, hand, wide_chunk), F32),
        pltpu.VMEM((6, quads - 1, hand, wide_chunk), BF16),
        pltpu.VMEM((6, quads - 1, hand, wide_chunk), BF16),
        pltpu.SemaphoreType.DMA((7,)),
        pltpu.SemaphoreType.DMA((4,)),
        pltpu.SemaphoreType.DMA((6,)),
        pltpu.SemaphoreType.DMA((6,)),
        pltpu.SemaphoreType.DMA((6, quads - 1)),
    ]
    ig, vg, gg, dgrad, small = pl.pallas_call(
        functools.partial(kernel, sp, dp, ratio),
        out_shape=(
            pltpu.VMEM((tokens, width), BF16),
            pltpu.VMEM((lines, lanes), F32),
            pltpu.VMEM((lines, lanes), F32),
            pltpu.VMEM((lines, lanes), F32),
            pltpu.VMEM((small_rows, chans), F32),
        ),
        in_specs=[hbm] * 9,
        out_specs=(vmem,) * 5,
        scratch_shapes=[
            pltpu.VMEM((tokens, width), BF16),
            pltpu.VMEM((tokens, width), BF16),
            pltpu.VMEM((width, chans), BF16),
            pltpu.VMEM((width, chans), BF16),
            pltpu.VMEM((chans, width), BF16),
            pltpu.VMEM((taps, chans), F32),
            pltpu.VMEM((1, chans), F32),
            pltpu.VMEM((1, chans), F32),
            pltpu.VMEM((1, chans), F32),
            dma((9,)),
            pltpu.VMEM(full, F32),
            pltpu.VMEM(full, F32),
            pltpu.VMEM((tokens + 4 * PAD, chans), F32),
            pltpu.VMEM(extended, F32),
            pltpu.VMEM(extended, F32),
            pltpu.VMEM(extended, F32),
            pltpu.VMEM(extended, BF16),
            pltpu.VMEM(full, BF16),
            pltpu.VMEM(full, BF16),
            pltpu.VMEM(turned_shape, BF16),
            pltpu.VMEM((2, tokens + 2 * PAD, 128), F32),
            pltpu.VMEM((4, dp, stat_rows, 128), F32),
            pltpu.VMEM(part_shape, F32),
            pltpu.VMEM(ring_shape, BF16),
            pltpu.VMEM(ring_shape, BF16),
            pltpu.VMEM((half, width), BF16),
            pltpu.VMEM((half, width), BF16),
            pltpu.VMEM((half, width), F32),
            pltpu.VMEM((bits_dp, half, width), BF16),
            pltpu.VMEM((bits_dp - 1, half, width), BF16),
            pltpu.VMEM((bits_sp + 1, small_rows, chans), F32),
            pltpu.VMEM((bits_sp, small_rows, chans), F32),
            dma((4,)),
            dma((4,)),
            dma((4,)),
            dma((4,)),
            dma((1,)),
            dma(ring_sems),
            dma((bits_dp + 1,)),
            dma((bits_dp, GROUPS)),
            dma((1,)),
            dma((1,)),
            dma((bits_sp,)),
            *pair_scratch,
        ],
        compiler_params=pltpu.CompilerParams(
            collective_id=0, has_side_effects=True, vmem_limit_bytes=MAIN
        ),
    )(
        normed_input,
        out_grad,
        value_weight,
        gate_weight,
        down_weight,
        conv_kernel,
        conv_bias[None, :],
        norm_gain[None, :],
        norm_shift[None, :],
    )
    row = jax.ShapeDtypeStruct((chans,), F32)
    return pl.pallas_call(
        functools.partial(finish, wide),
        out_shape=(
            jax.ShapeDtypeStruct(ig.shape, BF16),
            jax.ShapeDtypeStruct(vg.shape, F32),
            jax.ShapeDtypeStruct(gg.shape, F32),
            jax.ShapeDtypeStruct((chans, chunk), F32),
            jax.ShapeDtypeStruct((taps, chans), F32),
            row,
            row,
            row,
        ),
        in_specs=[vmem] * 5,
        out_specs=(hbm,) * 8,
        scratch_shapes=[
            pltpu.VMEM((lanes, lines), F32),
            pltpu.VMEM((lanes, lines), F32),
            pltpu.VMEM((taps, chans), F32),
            pltpu.VMEM((chans,), F32),
            pltpu.VMEM((chans,), F32),
            pltpu.VMEM((chans,), F32),
            dma((8,)),
        ],
        compiler_params=pltpu.CompilerParams(vmem_limit_bytes=FINISH),
    )(ig, vg, gg, dgrad, small)


def solution(mesh):
    in_specs = (
        P("sp", None),
        P("sp", None),
        P(None, "dp"),
        P(None, "dp"),
        P("dp", None),
        P(None, "dp"),
        P("dp"),
        P("dp"),
        P("dp"),
    )
    out_specs = (
        P("sp", None),
        P("sp", "dp"),
        P("sp", "dp"),
        P("dp", "sp"),
        P(None, "dp"),
        P("dp"),
        P("dp"),
        P("dp"),
    )
    return jax.shard_map(
        on_device, mesh=mesh, in_specs=in_specs, out_specs=out_specs, check_vma=False
    )
```

```python
import functools
import math

import jax
import jax.numpy as jnp
from jax import lax
from jax.experimental import pallas as pl
from jax.experimental.pallas import tpu as pltpu
from jax.sharding import PartitionSpec as P

EPS = 1e-05
F32 = jnp.float32
BF16 = jnp.bfloat16
MESH = pl.DeviceIdType.MESH
NN = (((1,), (0,)), ((), ()))
NT = (((1,), (1,)), ((), ()))
TN = (((0,), (0,)), ((), ()))
PAD = 16
ROWS = 32
SUBS = 2
GROUPS = 2
DIRECT = (0,)
CUTS = 2
MAIN = 61_900_000
FINISH = 16_000_000


def dot(a, b, numbers):
    return lax.dot_general(a, b, numbers, preferred_element_type=F32)


def split3(v):
    high = v.astype(BF16)
    rest = v - high.astype(F32)
    mid = rest.astype(BF16)
    return high, mid, (rest - mid.astype(F32)).astype(BF16)


def is_wide(chunk, chans):
    return chunk % 128 == 0 and chans % 32 == 0


def is_paired(sp, dp, chunk, chans):
    return is_wide(chunk, chans) and chans % 256 == 0 and sp % 4 == 0 and sp >= 8 and dp % 2 == 0


def kernel(
    sp,
    dp,
    ratio,
    x_hbm,
    og_hbm,
    wv_hbm,
    wg_hbm,
    wd_hbm,
    ck_hbm,
    bias_hbm,
    gain_hbm,
    shift_hbm,
    ig_out,
    vg_out,
    gg_out,
    dg_out,
    small_out,
    x,
    og,
    wv,
    wg,
    wd,
    ck,
    bias,
    gain,
    shift,
    load_sem,
    value,
    opening,
    glu,
    mixed,
    d_act,
    d_pad,
    act,
    dv,
    dg,
    turned,
    cols,
    stats,
    part,
    ring_src,
    ring_dst,
    ig_send,
    ig_recv,
    ig_own,
    ig_sum,
    ig_peer,
    small,
    small_recv,
    halo_send,
    halo_recv,
    stat_send,
    stat_recv,
    ring_send,
    ring_recv,
    ig_ssem,
    ig_rsem,
    give_rsem,
    small_ssem,
    small_rsem,
    xp,
    ogp,
    in_recv,
    lhs,
    x_send,
    x_recv,
    held,
    z_send,
    z_recv,
    z_send2,
    z_recv2,
    pair_sends,
    near_recv,
    in_rsem,
    x_rsem,
    z_rsem,
    cross_rsem,
):
    tokens, width = x.shape
    taps, chans = ck.shape
    channels = chans * dp
    reach = taps // 2
    chunk = width // sp
    wide = is_wide(chunk, chans)
    paired = is_paired(sp, dp, chunk, chans)
    lines = chans if wide else chunk
    strip = lines // (2 * SUBS)
    tile = min(256, width)
    s = lax.axis_index("sp")
    d = lax.axis_index("dp")
    bits_sp = sp.bit_length() - 1
    bits_dp = dp.bit_length() - 1

    def flip(i, bit):
        step = 1 << bit
        return i + step * (1 - 2 * lax.rem(lax.div(i, step), 2))

    def index_of(p):
        far = lax.div(p, sp // 2)
        return (1 - far) * 2 * p + far * (2 * sp - 1 - 2 * p)

    odd = lax.rem(s, 2)
    pos = (1 - odd) * lax.div(s, 2) + odd * (sp - 1 - lax.div(s, 2))
    ahead = index_of(lax.rem(pos + 1, sp))
    behind = index_of(lax.rem(pos + sp - 1, sp))

    loads = [
        pltpu.make_async_copy(src, dst, load_sem.at[at])
        for at, (src, dst) in enumerate(
            [
                (x_hbm, x),
                (wv_hbm, wv),
                (wg_hbm, wg),
                (og_hbm, og),
                (wd_hbm, wd),
                (ck_hbm, ck),
                (bias_hbm, bias),
                (gain_hbm, gain),
                (shift_hbm, shift),
            ]
        )
    ]
    for load in loads:
        load.start()

    barrier = pltpu.get_barrier_semaphore()
    peers = [ahead, behind, lax.rem(s + 1, sp), lax.rem(s + sp - 1, sp)]
    peers += [flip(s, bit) for bit in range(bits_sp)]
    quads = sp // 4
    if paired and quads > 2:
        peers += [lax.rem(s + 4 * far, sp) for far in range(1, quads)]
    for peer in peers:
        pl.semaphore_signal(barrier, inc=1, device_id={"sp": peer}, device_id_type=MESH)
    for off in range(1, dp):
        pl.semaphore_signal(
            barrier, inc=1, device_id={"dp": lax.rem(d + off, dp)}, device_id_type=MESH
        )

    for load in loads[:3]:
        load.wait()
    value_f, gate_f = dot(x[...], wv[...], NN), dot(x[...], wg[...], NN)
    value[...] = value_f.astype(BF16).astype(F32)
    opening[...] = gate_f.astype(BF16).astype(F32)

    def row_loop(fn, init=None, rows=ROWS, begin=0, end=tokens):
        def step(i, carry):
            return fn(pl.multiple_of(begin + i * rows, math.gcd(begin, rows)), carry)

        return lax.fori_loop(0, (end - begin) // rows, step, init)

    ext = tokens + 2 * PAD
    inner_rows = ext - 2 * ROWS
    big = 96 if inner_rows % 96 == 0 else ROWS
    own = pl.ds(PAD, tokens)

    def make_glu(r, _):
        here = pl.ds(r, ROWS)
        o = jax.nn.sigmoid(opening[here, :])
        opening[here, :] = o
        glu[pl.ds(r + 2 * PAD, ROWS), :] = value[here, :] * o

    row_loop(make_glu)
    pl.semaphore_wait(barrier, len(peers) + dp - 1)

    has_low, has_high = s > 0, s < sp - 1

    def halo_copies(buf, pad, at):
        up = pltpu.make_async_remote_copy(
            src_ref=buf.at[pl.ds(tokens, pad)],
            dst_ref=buf.at[pl.ds(0, pad)],
            send_sem=halo_send.at[at],
            recv_sem=halo_recv.at[at],
            device_id={"sp": lax.rem(s + 1, sp)},
            device_id_type=MESH,
        )
        down = pltpu.make_async_remote_copy(
            src_ref=buf.at[pl.ds(pad, pad)],
            dst_ref=buf.at[pl.ds(tokens + pad, pad)],
            send_sem=halo_send.at[at + 1],
            recv_sem=halo_recv.at[at + 1],
            device_id={"sp": lax.rem(s + sp - 1, sp)},
            device_id_type=MESH,
        )
        return up, down

    def halo_zero(buf, pad):
        @pl.when(s == 0)
        def _():
            buf[pl.ds(0, pad), :] = jnp.zeros((pad, chans), F32)

        @pl.when(s == sp - 1)
        def _():
            buf[pl.ds(tokens + pad, pad), :] = jnp.zeros((pad, chans), F32)

    def halo_start(buf, pad, at):
        up, down = halo_copies(buf, pad, at)
        pl.when(has_high)(up.start)
        pl.when(has_low)(down.start)
        halo_zero(buf, pad)

    def halo_wait(buf, pad, at):
        up, down = halo_copies(buf, pad, at)

        @pl.when(has_low)
        def _():
            up.wait_recv()
            down.wait_send()

        @pl.when(has_high)
        def _():
            down.wait_recv()
            up.wait_send()

    half = tokens // 2
    hand = chans // 2
    core = lax.rem(d, 2)
    these = pl.ds(pl.multiple_of(core * half, half), half)
    slots = [(far, other) for other in (1, 0) for far in range(quads)]
    held_rows, near_rows = (x, og), (xp, ogp)
    in_bits, mid_bits = (1, 0), (0, 1)

    def columns_of(who, far, other, kind):
        index = lax.rem(who + 4 * far, sp)
        if other:
            index = flip(index, mid_bits[kind])
        return pl.ds(pl.multiple_of(index * chunk, chunk), chunk)

    def slot_of(far, other):
        return pl.ds((2 * far + other) * chunk, chunk)

    def send_to(at, src, dst, recv_sem, where):
        return pltpu.make_async_remote_copy(
            src_ref=src,
            dst_ref=dst,
            send_sem=pair_sends.at[at],
            recv_sem=recv_sem,
            device_id=where,
            device_id_type=MESH,
        )

    def near_start(kind, those):
        there = flip(s, in_bits[kind])
        for far, other in those if paired else ():
            send_to(
                kind,
                held_rows[kind].at[these, columns_of(there, far, other, kind)],
                near_rows[kind].at[these, slot_of(far, other)],
                near_recv.at[kind],
                {"sp": there},
            ).start()

    def near_all(kind, stage):
        where = {"dp": flip(d, 0)} if stage else {"sp": flip(s, in_bits[kind])}
        rows = near_rows[kind].at[these]
        at = kind + 2 * stage
        return send_to(at, rows, rows, near_recv.at[at], where)

    halo_start(glu, 2 * PAD, 0)
    for load in loads[3:]:
        load.wait()
    d_act[own, :] = dot(og[...], wd[...], NT)
    halo_start(d_act, PAD, 2)

    span = ROWS + 2 * PAD

    def shifted(buf, r, offset):
        window = buf[pl.ds(r, span), :]
        return pltpu.roll(window, span - offset, 0) if offset else window

    def slide(buf, r, offset_of, acc):
        for low in range(8):
            those = [tap for tap in range(taps) if offset_of(tap) % 8 == low]
            if those:
                window = shifted(buf, r, low)
                for tap in those:
                    high = offset_of(tap) - low
                    acc = acc + ck[tap : tap + 1, :] * window[high : high + ROWS]
        return acc

    def conv(r, _):
        acc = jnp.zeros((ROWS, chans), F32) + bias[...]
        mixed[pl.ds(r, ROWS), :] = slide(glu, r, lambda tap: tap + PAD - reach, acc)

    ones = jnp.ones((16, chans), BF16)
    eye = (
        lax.rem(lax.broadcasted_iota(jnp.int32, (24, 128), 0), 8)
        == lax.broadcasted_iota(jnp.int32, (24, 128), 1)
    ).astype(BF16)
    edges = ((0, ROWS), (ext - ROWS, ROWS))
    regions = (((ROWS, inner_rows),), edges)

    def pieces_of(region):
        count = sum(size for _, size in regions[region])
        return [(at, min(128, count - at)) for at in range(0, count, 128)]

    def rows_of(buf, region):
        got = [buf[pl.ds(first, size), :] for first, size in regions[region]]
        return got[0] if len(got) == 1 else jnp.concatenate(got, axis=0)

    def row_sums(v):
        a, b, c = (dot(ones, term, NT) for term in split3(v))
        return a + b + c

    def columns(at, region, one, two):
        line = lax.broadcasted_iota(jnp.int32, (8, one.shape[1]), 0)
        both = jnp.where(line == 0, one, jnp.where(line == 1, two, 0.0))
        terms = [term.astype(F32) for term in split3(both)]
        got = dot(jnp.concatenate(terms, axis=0).astype(BF16), eye, TN)
        done = 0
        for first, size in regions[region]:
            cols[at, pl.ds(first, size), :] = got[done : done + size]
            done += size

    def stat_copy(at, off):
        return pltpu.make_async_remote_copy(
            src_ref=stats.at[at, 0],
            dst_ref=stats.at[at, off],
            send_sem=stat_send.at[at],
            recv_sem=stat_recv.at[at],
            device_id={"dp": lax.rem(d + off, dp)},
            device_id_type=MESH,
        )

    def stat_all(at):
        every = stats.at[at, pl.ds(1, dp - 1)]
        return pltpu.make_async_remote_copy(
            src_ref=every,
            dst_ref=every,
            send_sem=stat_send.at[at],
            recv_sem=stat_recv.at[at],
            device_id={"dp": lax.rem(d + 1, dp)},
            device_id_type=MESH,
        )

    def stat_start(at, region, one, two):
        pieces = pieces_of(region)
        stats[at, 0] = jnp.zeros(stats.shape[2:], F32)
        for first, sums in ((0, row_sums(one)), (len(pieces), row_sums(two))):
            for j, (begin, size) in enumerate(pieces):
                stats[at, 0, first + j : first + j + 1, 0:size] = sums[0:1, begin : begin + size]
        for off in range(1, dp):
            stat_copy(at, off).start()

    def stat_wait(at, region):
        pieces = pieces_of(region)
        stat_all(at).wait_recv()
        total = stats[at, 0]
        for off in range(1, dp):
            total = total + stats[at, off]
        total = total * (1.0 / channels)
        return tuple(
            jnp.concatenate(
                [total[first + j : first + j + 1, 0:size] for j, (_, size) in enumerate(pieces)],
                axis=1,
            )
            for first in (0, len(pieces))
        )

    def moments_start(region):
        v = rows_of(mixed, region)
        stat_start(region, region, v, v * v)

    def moments_wait(region):
        mean, square = stat_wait(region, region)
        columns(0, region, mean, lax.rsqrt(square - mean * mean + EPS))

    def second_start(region):
        v = rows_of(d_act, region)
        stat_start(2 + region, region, v, v * rows_of(mixed, region))

    def second_wait(region):
        columns(1, region, *stat_wait(2 + region, region))

    row_loop(conv, begin=ROWS, end=ext - ROWS)
    moments_start(0)
    halo_wait(glu, 2 * PAD, 0)
    near_start(1, slots)
    near_start(0, slots)

    def conv_edge(i, _):
        conv(pl.multiple_of(i * (ext - ROWS), ROWS), None)

    lax.fori_loop(0, 2, conv_edge, None)
    moments_start(1)

    def norm_rows(r, rows):
        here = pl.ds(r, rows)
        col = cols[0, here, :]
        centred = (mixed[here, :] - col[:, 0:1]) * col[:, 1:2]
        normed = centred * gain[...] + shift[...]
        sig = jax.nn.sigmoid(normed)
        act[here, :] = (normed * sig).astype(BF16)
        d_normed = d_act[here, :] * sig * (1.0 + normed * (1.0 - sig))
        mixed[here, :] = centred
        d_act[here, :] = d_normed * gain[...]
        return d_normed * centred, d_normed

    def down(v):
        return jnp.sum(v, axis=0, keepdims=True)

    def norm(r, carry):
        return tuple(had + down(v) for had, v in zip(carry, norm_rows(r, big)))

    zero = jnp.zeros((1, chans), F32)
    moments_wait(0)
    sums = row_loop(norm, (zero, zero), big, ROWS, ext - ROWS)
    second_start(0)
    halo_wait(d_act, PAD, 2)
    moments_wait(1)
    kept = (slice(PAD, ROWS), slice(0, ROWS - PAD))
    for (first, size), keep in zip(edges, kept):
        sums = tuple(had + down(v[keep]) for had, v in zip(sums, norm_rows(first, size)))
    gain_sum, shift_sum = sums
    second_start(1)

    def several(count, fn):
        if count <= 8:
            for i in range(count):
                fn(i)
        else:
            lax.fori_loop(0, count, lambda i, _: fn(i), None)

    def grad_tile(at, rows, off):
        index = index_of(lax.rem(pos + off + 2 * sp, sp))
        those = pl.ds(pl.multiple_of(index * chunk, chunk), chunk)
        part[at, pl.ds(pl.multiple_of(index * lines, lines), lines), :] = dot(
            turned[at], rows[:, those], NN
        )

    def grad_first(at, rows, factor):
        if wide:
            turned[at] = factor.T
            grad_tile(at, rows, -1)
            grad_tile(at, rows, 1)
            return

        def step(i, _):
            here = pl.ds(pl.multiple_of(i * tile, tile), tile)
            part[at, here, :] = dot(rows[:, here], factor, TN)

        lax.fori_loop(0, width // tile, step, None)

    def grad_rest(at, rows):
        if wide:
            several(sp - 2, lambda i: grad_tile(at, rows, (i + 2) % (sp - 1)))

    streams = [
        (at, 2 * sub + (way < 0), way) for at in range(3) for sub in range(SUBS) for way in (1, -1)
    ]
    early = [i for i, (at, _, _) in enumerate(streams) if at == 2]
    late = [i for sub in range(SUBS) for i, (at, place, _) in enumerate(streams) if at < 2 and place // 2 == sub]

    def late_of(at):
        return [i for i in late if streams[i][0] == at]

    def piece(stream, p):
        at, place, _ = streams[stream]
        first = index_of(lax.rem(p + 2 * sp, sp)) * lines + place * strip
        return part[at, pl.ds(pl.multiple_of(first, strip), strip), :]

    def ring_copy(stream, k):
        return pltpu.make_async_remote_copy(
            src_ref=ring_src.at[stream, k],
            dst_ref=ring_dst.at[stream, k],
            send_sem=ring_send.at[0],
            recv_sem=ring_recv.at[stream, k],
            device_id={"sp": ahead if streams[stream][2] == 1 else behind},
            device_id_type=MESH,
        )

    def ring_step(k, which):
        for stream in which:
            way = streams[stream][2]
            mine = piece(stream, pos - way * (1 + k))
            if not (isinstance(k, int) and k == 0):
                ring_copy(stream, k - 1).wait_recv()
                mine = mine + ring_dst[stream, k - 1].astype(F32)
            ring_src[stream, k] = mine.astype(BF16)
            ring_copy(stream, k).start()

    def ring_end(which, outs):
        for stream in which:
            at, place, _ = streams[stream]
            ring_copy(stream, sp - 2).wait_recv()
            outs[at][pl.ds(place * strip, strip), :] = ratio * (
                piece(stream, pos) + ring_dst[stream, sp - 2].astype(F32)
            )

    blocks = [(at, hand * place) for at in (2, 0, 1) for place in range(2)]

    def kind_of(n):
        return int(blocks[n][0] == 2)

    def factor_of(n):
        at, first = blocks[n]
        those = pl.ds(first, hand)
        return (dv, dg, act)[at].at[own if at == 2 else pl.ds(0, tokens), those]

    def in_copy(n):
        where = {"sp": flip(s, in_bits[kind_of(n)])}
        return send_to(4, factor_of(n), in_recv.at[n], in_rsem.at[n], where)

    strips = [pl.ds(cut * (hand // CUTS), hand // CUTS) for cut in range(CUTS)]

    def mid_copy(n, cut):
        where = {"sp": flip(s, mid_bits[kind_of(n)])}
        at, far = (7, 0) if n in DIRECT else (5, slice(None))
        src, dst = x_send.at[n, far, strips[cut]], x_recv.at[n, far, strips[cut]]
        return send_to(at, src, dst, x_rsem.at[n, cut], where)

    def cross_copy(n, far):
        at = DIRECT.index(n)
        where = {"sp": flip(lax.rem(s + 4 * far, sp), mid_bits[kind_of(n)])}
        return send_to(
            8, z_send2.at[at, far - 1], z_recv2.at[at, far - 1], cross_rsem.at[at, far - 1], where
        )

    def far_copy(n, far, cut):
        where = {"sp": lax.rem(s + 4 * far, sp)}
        src, dst = z_send.at[n, far - 1, strips[cut]], z_recv.at[n, far - 1, strips[cut]]
        return send_to(6, src, dst, z_rsem.at[n, far - 1, cut], where)

    def far_copies(n, far):
        return [far_copy(n, far, cut) for cut in range(CUTS)]

    def product(n):
        kind = kind_of(n)
        in_copy(n).wait_recv()
        lhs[...] = jnp.concatenate([factor_of(n)[...], in_recv[n]], axis=0).T
        direct = n in DIRECT
        for far, other in sorted(slots, key=lambda at: -at[0]) if direct else slots:
            mine = held_rows[kind][:, columns_of(s, far, other, kind)]
            rows = jnp.concatenate([mine, near_rows[kind][:, slot_of(far, other)]], axis=0)
            got = dot(lhs[...], rows, NN)
            if direct and far:
                sent = got.astype(BF16)
                if other:
                    z_send2[DIRECT.index(n), far - 1] = sent
                else:
                    z_send[n, far - 1] = sent
                for copy in [cross_copy(n, far)] if other else far_copies(n, far):
                    copy.start()
            elif other:
                x_send[n, far] = got.astype(BF16)
            else:
                held[n, far] = got
            if (far, other) == (0 if direct else quads - 1, 1):
                for cut in range(CUTS):
                    mid_copy(n, cut).start()

    def meet(n):
        for cut, rows in enumerate(strips):
            mid_copy(n, cut).wait_recv()
            for far in () if n in DIRECT else range(1, quads):
                got = held[n, far, rows, :] + x_recv[n, far, rows, :].astype(F32)
                z_send[n, far - 1, rows, :] = got.astype(BF16)
                far_copy(n, far, cut).start()
            held[n, 0, rows, :] = held[n, 0, rows, :] + x_recv[n, 0, rows, :].astype(F32)

    def settle(n, outs):
        at, first = blocks[n]
        total = held[n, 0]
        for far in range(1, quads):
            for copy in far_copies(n, far):
                copy.wait_recv()
            total = total + z_recv[n, far - 1].astype(F32)
            if n in DIRECT:
                cross_copy(n, far).wait_recv()
                total = total + z_recv2[DIRECT.index(n), far - 1].astype(F32)
        outs[at][pl.ds(first, hand), :] = ratio * total

    if paired:
        for n in range(2):
            in_copy(n).start()
    else:
        grad_first(2, og, act[own, :])
        ring_step(0, early)
        grad_rest(2, og)

    def back_rows(r, rows):
        here = pl.ds(r, rows)
        col, back = cols[0, here, :], cols[1, here, :]
        d_mixed = col[:, 1:2] * (d_act[here, :] - back[:, 0:1] - mixed[here, :] * back[:, 1:2])
        d_pad[here, :] = d_mixed
        return d_mixed

    def norm_back(r, bias_sum):
        return bias_sum + down(back_rows(r, big))

    def conv_back(r, _):
        here = pl.ds(r, ROWS)
        acc = jnp.zeros((ROWS, chans), F32)
        acc = slide(d_pad, r, lambda tap: PAD + reach - tap, acc)
        o = opening[here, :]
        grad = acc * o
        dv[here, :] = grad.astype(BF16)
        dg[here, :] = (grad * value[here, :] * (1.0 - o)).astype(BF16)

    second_wait(0)
    bias_sum = row_loop(norm_back, zero, big, ROWS, ext - ROWS)
    row_loop(conv_back, begin=ROWS, end=tokens - ROWS)
    second_wait(1)
    for (first, size), keep in zip(edges, kept):
        bias_sum = bias_sum + down(back_rows(first, size)[keep])
    halo_zero(d_pad, PAD)

    def back_edge(i, _):
        conv_back(pl.multiple_of(i * (tokens - ROWS), ROWS), None)

    lax.fori_loop(0, 2, back_edge, None)
    if not paired:
        ring_step(1, early)
    if paired:
        for n in range(2, 6):
            in_copy(n).start()
    else:
        grad_first(0, x, dv[...])
        ring_step(0, late_of(0))
        grad_first(1, x, dg[...])
        ring_step(0, late_of(1))
        grad_rest(0, x)
        grad_rest(1, x)
        ring_step(2, early)

    mine = pl.multiple_of(lax.rem(d, 2) * half, half)
    other = pl.multiple_of((1 - lax.rem(d, 2)) * half, half)
    group = width // GROUPS

    def ig_copy(at, g, src, dst, bit):
        return pltpu.make_async_remote_copy(
            src_ref=src,
            dst_ref=dst,
            send_sem=ig_ssem.at[at],
            recv_sem=give_rsem.at[0] if at == bits_dp else ig_rsem.at[at, g],
            device_id={"dp": flip(d, bit)},
            device_id_type=MESH,
        )

    def of_group(g):
        return pl.ds(g * group, group)

    def pair_copy(g):
        return ig_copy(0, g, ig_send.at[:, of_group(g)], ig_recv.at[:, of_group(g)], 0)

    def y_copy(bit, g):
        return ig_copy(
            bit, g, ig_sum.at[bit - 1, :, of_group(g)], ig_peer.at[bit - 1, :, of_group(g)], bit
        )

    final = bits_dp - 1

    def give_copy(g):
        return ig_copy(
            bits_dp,
            g,
            ig_sum.at[final, :, of_group(g)],
            ig_out.at[pl.ds(mine, half), of_group(g)],
            0,
        )

    small[0] = jnp.zeros(small.shape[1:], F32)

    def taps_grad(low):
        those = [
            [tap for tap in range(taps) if (tap + PAD - reach) % 8 == low + at] for at in range(2)
        ]

        def taps_sum(r, sums):
            grad = d_pad[pl.ds(r + PAD, ROWS), :]
            new = []
            for at in range(2):
                window = shifted(glu, r + PAD, low + at)
                for tap in those[at]:
                    high = tap + PAD - reach - low - at
                    prod = grad * window[high : high + ROWS]
                    acc = sums[len(new)]
                    for row in range(0, ROWS, 8):
                        acc = acc + prod[row : row + 8]
                    new.append(acc)
            return tuple(new)

        flat = those[0] + those[1]
        sums = row_loop(taps_sum, tuple(jnp.zeros((8, chans), F32) for _ in flat))
        for acc, tap in zip(sums, flat):
            small[0, tap : tap + 1, :] = jnp.sum(acc, axis=0, keepdims=True) * ratio

    part_rows = small.shape[1] // 2
    my_rows = pl.ds(pl.multiple_of(lax.rem(s, 2) * part_rows, 8), part_rows)

    def small_copy(turn):
        if turn == 0:
            src, dst, bit = small.at[0], small_recv.at[0], 0
        elif turn < bits_sp:
            src, dst, bit = small.at[turn, my_rows], small_recv.at[turn, my_rows], turn
        else:
            src, dst, bit = small.at[turn, my_rows], small.at[turn, my_rows], 0
        return pltpu.make_async_remote_copy(
            src_ref=src,
            dst_ref=dst,
            send_sem=small_ssem.at[min(turn, 1)],
            recv_sem=small_rsem.at[turn],
            device_id={"sp": flip(s, bit)},
            device_id_type=MESH,
        )

    def small_first():
        small[0, taps : taps + 1, :] = bias_sum * ratio
        small[0, taps + 1 : taps + 2, :] = gain_sum * ratio
        small[0, taps + 2 : taps + 3, :] = shift_sum * ratio
        small_copy(0).start()

    def small_next(turn):
        small_copy(turn).wait_recv()
        if turn < bits_sp:
            those = my_rows if turn else slice(None)
            small[turn + 1, those, :] = small[turn, those, :] + small_recv[turn, those, :]
            small_copy(turn + 1).start()

    def taps_half(lows):
        for low in lows:
            taps_grad(low)

    both_v = jnp.concatenate([dv[pl.ds(other, half), :], dv[pl.ds(mine, half), :]], axis=0)
    both_g = jnp.concatenate([dg[pl.ds(other, half), :], dg[pl.ds(mine, half), :]], axis=0)
    size = min(tile, group)
    for g in range(GROUPS):
        for begin in range(g * group, (g + 1) * group, size):
            here = pl.ds(begin, size)
            got = dot(both_v, wv[here, :], NT) + dot(both_g, wg[here, :], NT)
            ig_send[:, here] = got[:half].astype(BF16)
            ig_own[:, here] = got[half:]
        pair_copy(g).start()

    def pair_sums():
        for g in range(GROUPS):
            pair_copy(g).wait_recv()
            here = of_group(g)
            ig_sum[0, :, here] = (ig_own[:, here] + ig_recv[:, here].astype(F32)).astype(BF16)
            if bits_dp > 1:
                y_copy(1, g).start()

    if paired:
        for kind in (1, 0):
            near_all(kind, 0).wait_recv()
            near_all(kind, 1).start()
        taps_half((0, 2, 4, 6))
        small_first()
    pair_sums()
    fixed = min(sp - 2, 6)
    if paired:
        near_all(0, 1).wait_recv()
        product(2)
        product(3)
        small_next(0)
        near_all(1, 1).wait_recv()
        product(0)
        product(1)
        product(4)
        product(5)
        meet(2)
        small_next(1)
        meet(3)
        meet(0)
        meet(4)
        meet(1)
        meet(5)
        small_next(2)
        for turn in range(3, bits_sp + 1):
            small_next(turn)
        fixed = 0
    for k in range(1, fixed + 1):
        ring_step(k, late)
        if k + 2 <= sp - 2:
            ring_step(k + 2, early)
        if k == 1:
            taps_half((0, 2))
        if k == 2:
            taps_half((4, 6))
            small_first()
        if k > 2 and k - 3 <= bits_sp:
            small_next(k - 3)
    for turn in range(max(fixed - 2, 0), bits_sp + 1 if fixed else 0):
        small_next(turn)
    if sp - 2 > fixed and fixed:

        def both(k, _):
            ring_step(k, late)
            ring_step(k + 2, early)

        lax.fori_loop(fixed + 1, sp - 3, both, None)
        ring_step(sp - 3, late)
        ring_step(sp - 2, late)

    for bit in range(1, bits_dp):
        for g in range(GROUPS):
            y_copy(bit, g).wait_recv()
            here = of_group(g)
            got = ig_sum[bit - 1, :, here].astype(F32) + ig_peer[bit - 1, :, here].astype(F32)
            ig_sum[bit, :, here] = got.astype(BF16)
            if bit + 1 < bits_dp:
                y_copy(bit + 1, g).start()
            else:
                give_copy(g).start()
    if bits_dp == 1:
        for g in range(GROUPS):
            give_copy(g).start()
    ig_out[pl.ds(mine, half), :] = ig_sum[final]
    small_out[...] = small[bits_sp]
    if paired:
        for n in (2, 3, 0, 4, 1, 5):
            settle(n, (vg_out, gg_out, dg_out))
        for kind in range(2):
            near_all(kind, 0).wait_send()
            near_all(kind, 1).wait_send()
        waits = [(4, in_recv), (5, x_send.at[pl.ds(0, 6 - len(DIRECT))]), (6, z_send)]
        if DIRECT:
            waits += [(7, x_send.at[pl.ds(0, len(DIRECT)), 0]), (8, z_send2)]
        for at, ref in waits:
            send_to(at, ref, ref, near_recv.at[0], {"sp": flip(s, 0)}).wait_send()
    else:
        ring_end(early + late, (vg_out, gg_out, dg_out))
        pltpu.make_async_remote_copy(
            src_ref=ring_src,
            dst_ref=ring_dst,
            send_sem=ring_send.at[0],
            recv_sem=ring_recv.at[0, 0],
            device_id={"sp": ahead},
            device_id_type=MESH,
        ).wait_send()

    ig_copy(0, 0, ig_send, ig_recv, 0).wait_send()
    for bit in range(1, bits_dp):
        ig_copy(bit, 0, ig_sum.at[bit - 1], ig_peer.at[bit - 1], bit).wait_send()
    ig_copy(bits_dp, 0, ig_sum.at[final], ig_out.at[pl.ds(mine, half)], 0).wait()
    for at in range(4):
        stat_all(at).wait_send()
    for at, sent in ((0, small.at[0]), (1, small.at[pl.ds(1, bits_sp), my_rows])):
        pltpu.make_async_remote_copy(
            src_ref=sent,
            dst_ref=sent,
            send_sem=small_ssem.at[at],
            recv_sem=small_rsem.at[0],
            device_id={"sp": flip(s, 0)},
            device_id_type=MESH,
        ).wait_send()


def finish(
    wide, ig, vg, gg, dgrad, small, ig_o, vg_o, gg_o, dg_o, k_o, b_o, g_o, s_o,
    t0, t1, k_v, b_v, g_v, s_v, sem,
):
    copies = []

    def send(src, dst):
        copies.append(pltpu.make_async_copy(src, dst, sem.at[len(copies)]))
        copies[-1].start()

    send(ig, ig_o)
    turn = [(vg, vg_o), (gg, gg_o)] if wide else [(dgrad, dg_o)]
    keep = [(dgrad, dg_o)] if wide else [(vg, vg_o), (gg, gg_o)]
    for src, dst in keep:
        send(src, dst)
    taps = k_o.shape[0]
    k_v[...] = small[0:taps, :]
    send(k_v, k_o)
    for at, (held, out) in enumerate(((b_v, b_o), (g_v, g_o), (s_v, s_o))):
        held[...] = small[taps + at, :]
        send(held, out)
    for (src, dst), held in zip(turn, (t0, t1)):
        held[...] = src[...].T
        send(held, dst)
    for copy in copies:
        copy.wait()


def on_device(
    normed_input,
    out_grad,
    value_weight,
    gate_weight,
    down_weight,
    conv_kernel,
    conv_bias,
    norm_gain,
    norm_shift,
):
    tokens, width = normed_input.shape
    taps, chans = conv_kernel.shape
    sp, dp = lax.axis_size("sp"), lax.axis_size("dp")
    ratio = 1.0 / math.sqrt(tokens * sp)
    chunk = width // sp
    bits_sp, bits_dp = sp.bit_length() - 1, dp.bit_length() - 1
    small_rows = -(-(taps + 3) // 16) * 16
    half = tokens // 2
    full, extended = (tokens, chans), (tokens + 2 * PAD, chans)
    vmem = pl.BlockSpec(memory_space=pltpu.VMEM)
    hbm = pl.BlockSpec(memory_space=pltpu.HBM)
    dma = pltpu.SemaphoreType.DMA
    wide = is_wide(chunk, chans)
    lines, lanes = (chans, chunk) if wide else (chunk, chans)
    stat_rows = -(-2 * -(-tokens // 128) // 8) * 8
    paired = is_paired(sp, dp, chunk, chans)
    if paired:
        ring_shape, ring_sems, part_shape, turned_shape = (1, 1, 16, 128), (1, 1), (1, 8, 128), (1, 16, 128)
    else:
        count = 3 * 2 * SUBS
        ring_shape, ring_sems = (count, sp - 1, lines // (2 * SUBS), lanes), (count, sp - 1)
        part_shape, turned_shape = (3, sp * lines, lanes), (3, chans, tokens)
    quads, hand = (sp // 4, chans // 2) if paired else (2, 16)
    near, wide_chunk = (tokens, chunk) if paired else (16, 128)
    pair_scratch = [
        pltpu.VMEM((near, 2 * quads * wide_chunk), BF16),
        pltpu.VMEM((near, 2 * quads * wide_chunk), BF16),
        pltpu.VMEM((6, near, hand), BF16),
        pltpu.VMEM((hand, 2 * near), BF16),
        pltpu.VMEM((6, quads, hand, wide_chunk), BF16),
        pltpu.VMEM((6, quads, hand, wide_chunk), BF16),
        pltpu.VMEM((6, quads, hand, wide_chunk), F32),
        pltpu.VMEM((6, quads - 1, hand, wide_chunk), BF16),
        pltpu.VMEM((6, quads - 1, hand, wide_chunk), BF16),
        pltpu.VMEM((max(len(DIRECT), 1), quads - 1, hand, wide_chunk), BF16),
        pltpu.VMEM((max(len(DIRECT), 1), quads - 1, hand, wide_chunk), BF16),
        pltpu.SemaphoreType.DMA((9,)),
        pltpu.SemaphoreType.DMA((4,)),
        pltpu.SemaphoreType.DMA((6,)),
        pltpu.SemaphoreType.DMA((6, CUTS)),
        pltpu.SemaphoreType.DMA((6, quads - 1, CUTS)),
        pltpu.SemaphoreType.DMA((max(len(DIRECT), 1), quads - 1)),
    ]
    ig, vg, gg, dgrad, small = pl.pallas_call(
        functools.partial(kernel, sp, dp, ratio),
        out_shape=(
            pltpu.VMEM((tokens, width), BF16),
            pltpu.VMEM((lines, lanes), F32),
            pltpu.VMEM((lines, lanes), F32),
            pltpu.VMEM((lines, lanes), F32),
            pltpu.VMEM((small_rows, chans), F32),
        ),
        in_specs=[hbm] * 9,
        out_specs=(vmem,) * 5,
        scratch_shapes=[
            pltpu.VMEM((tokens, width), BF16),
            pltpu.VMEM((tokens, width), BF16),
            pltpu.VMEM((width, chans), BF16),
            pltpu.VMEM((width, chans), BF16),
            pltpu.VMEM((chans, width), BF16),
            pltpu.VMEM((taps, chans), F32),
            pltpu.VMEM((1, chans), F32),
            pltpu.VMEM((1, chans), F32),
            pltpu.VMEM((1, chans), F32),
            dma((9,)),
            pltpu.VMEM(full, F32),
            pltpu.VMEM(full, F32),
            pltpu.VMEM((tokens + 4 * PAD, chans), F32),
            pltpu.VMEM(extended, F32),
            pltpu.VMEM(extended, F32),
            pltpu.VMEM(extended, F32),
            pltpu.VMEM(extended, BF16),
            pltpu.VMEM(full, BF16),
            pltpu.VMEM(full, BF16),
            pltpu.VMEM(turned_shape, BF16),
            pltpu.VMEM((2, tokens + 2 * PAD, 128), F32),
            pltpu.VMEM((4, dp, stat_rows, 128), F32),
            pltpu.VMEM(part_shape, F32),
            pltpu.VMEM(ring_shape, BF16),
            pltpu.VMEM(ring_shape, BF16),
            pltpu.VMEM((half, width), BF16),
            pltpu.VMEM((half, width), BF16),
            pltpu.VMEM((half, width), F32),
            pltpu.VMEM((bits_dp, half, width), BF16),
            pltpu.VMEM((bits_dp - 1, half, width), BF16),
            pltpu.VMEM((bits_sp + 1, small_rows, chans), F32),
            pltpu.VMEM((bits_sp, small_rows, chans), F32),
            dma((4,)),
            dma((4,)),
            dma((4,)),
            dma((4,)),
            dma((1,)),
            dma(ring_sems),
            dma((bits_dp + 1,)),
            dma((bits_dp, GROUPS)),
            dma((1,)),
            dma((2,)),
            dma((bits_sp + 1,)),
            *pair_scratch,
        ],
        compiler_params=pltpu.CompilerParams(
            collective_id=0, has_side_effects=True, vmem_limit_bytes=MAIN
        ),
    )(
        normed_input,
        out_grad,
        value_weight,
        gate_weight,
        down_weight,
        conv_kernel,
        conv_bias[None, :],
        norm_gain[None, :],
        norm_shift[None, :],
    )
    row = jax.ShapeDtypeStruct((chans,), F32)
    return pl.pallas_call(
        functools.partial(finish, wide),
        out_shape=(
            jax.ShapeDtypeStruct(ig.shape, BF16),
            jax.ShapeDtypeStruct(vg.shape, F32),
            jax.ShapeDtypeStruct(gg.shape, F32),
            jax.ShapeDtypeStruct((chans, chunk), F32),
            jax.ShapeDtypeStruct((taps, chans), F32),
            row,
            row,
            row,
        ),
        in_specs=[vmem] * 5,
        out_specs=(hbm,) * 8,
        scratch_shapes=[
            pltpu.VMEM((lanes, lines), F32),
            pltpu.VMEM((lanes, lines), F32),
            pltpu.VMEM((taps, chans), F32),
            pltpu.VMEM((chans,), F32),
            pltpu.VMEM((chans,), F32),
            pltpu.VMEM((chans,), F32),
            dma((8,)),
        ],
        compiler_params=pltpu.CompilerParams(vmem_limit_bytes=FINISH),
    )(ig, vg, gg, dgrad, small)


def solution(mesh):
    in_specs = (
        P("sp", None),
        P("sp", None),
        P(None, "dp"),
        P(None, "dp"),
        P("dp", None),
        P(None, "dp"),
        P("dp"),
        P("dp"),
        P("dp"),
    )
    out_specs = (
        P("sp", None),
        P("sp", "dp"),
        P("sp", "dp"),
        P("dp", "sp"),
        P(None, "dp"),
        P("dp"),
        P("dp"),
        P("dp"),
    )
    return jax.shard_map(
        on_device, mesh=mesh, in_specs=in_specs, out_specs=out_specs, check_vma=False
    )
```

```python
import functools
import math

import jax
import jax.numpy as jnp
from jax import lax
from jax.experimental import pallas as pl
from jax.experimental.pallas import tpu as pltpu
from jax.sharding import PartitionSpec as P

EPS = 1e-05
F32 = jnp.float32
BF16 = jnp.bfloat16
MESH = pl.DeviceIdType.MESH
NN = (((1,), (0,)), ((), ()))
NT = (((1,), (1,)), ((), ()))
TN = (((0,), (0,)), ((), ()))
PAD = 16
ROWS = 32
SUBS = 2
GROUPS = 2
DIRECT = (0,)
CUTS = 1
MAIN = 61_900_000
FINISH = 16_000_000


def dot(a, b, numbers):
    return lax.dot_general(a, b, numbers, preferred_element_type=F32)


def split3(v):
    high = v.astype(BF16)
    rest = v - high.astype(F32)
    mid = rest.astype(BF16)
    return high, mid, (rest - mid.astype(F32)).astype(BF16)


def is_wide(chunk, chans):
    return chunk % 128 == 0 and chans % 32 == 0


def is_paired(sp, dp, chunk, chans):
    return is_wide(chunk, chans) and chans % 256 == 0 and sp % 4 == 0 and sp >= 8 and dp % 2 == 0


def kernel(
    sp,
    dp,
    ratio,
    x_hbm,
    og_hbm,
    wv_hbm,
    wg_hbm,
    wd_hbm,
    ck_hbm,
    bias_hbm,
    gain_hbm,
    shift_hbm,
    ig_out,
    vg_out,
    gg_out,
    dg_out,
    small_out,
    x,
    og,
    wv,
    wg,
    wd,
    ck,
    bias,
    gain,
    shift,
    load_sem,
    value,
    opening,
    glu,
    mixed,
    d_act,
    d_pad,
    act,
    dv,
    dg,
    turned,
    cols,
    stats,
    part,
    ring_src,
    ring_dst,
    ig_send,
    ig_recv,
    ig_own,
    ig_sum,
    ig_peer,
    small,
    small_recv,
    halo_send,
    halo_recv,
    stat_send,
    stat_recv,
    ring_send,
    ring_recv,
    ig_ssem,
    ig_rsem,
    give_rsem,
    small_ssem,
    small_rsem,
    xp,
    ogp,
    in_recv,
    lhs,
    x_send,
    x_recv,
    held,
    z_send,
    z_recv,
    z_send2,
    z_recv2,
    pair_sends,
    near_recv,
    in_rsem,
    x_rsem,
    z_rsem,
    cross_rsem,
):
    tokens, width = x.shape
    taps, chans = ck.shape
    channels = chans * dp
    reach = taps // 2
    chunk = width // sp
    wide = is_wide(chunk, chans)
    paired = is_paired(sp, dp, chunk, chans)
    lines = chans if wide else chunk
    strip = lines // (2 * SUBS)
    tile = min(256, width)
    s = lax.axis_index("sp")
    d = lax.axis_index("dp")
    bits_sp = sp.bit_length() - 1
    bits_dp = dp.bit_length() - 1

    def flip(i, bit):
        step = 1 << bit
        return i + step * (1 - 2 * lax.rem(lax.div(i, step), 2))

    def index_of(p):
        far = lax.div(p, sp // 2)
        return (1 - far) * 2 * p + far * (2 * sp - 1 - 2 * p)

    odd = lax.rem(s, 2)
    pos = (1 - odd) * lax.div(s, 2) + odd * (sp - 1 - lax.div(s, 2))
    ahead = index_of(lax.rem(pos + 1, sp))
    behind = index_of(lax.rem(pos + sp - 1, sp))

    loads = [
        pltpu.make_async_copy(src, dst, load_sem.at[at])
        for at, (src, dst) in enumerate(
            [
                (x_hbm, x),
                (wv_hbm, wv),
                (wg_hbm, wg),
                (og_hbm, og),
                (wd_hbm, wd),
                (ck_hbm, ck),
                (bias_hbm, bias),
                (gain_hbm, gain),
                (shift_hbm, shift),
            ]
        )
    ]
    for load in loads[:3]:
        load.start()

    barrier = pltpu.get_barrier_semaphore()
    peers = [ahead, behind, lax.rem(s + 1, sp), lax.rem(s + sp - 1, sp)]
    peers += [flip(s, bit) for bit in range(bits_sp)]
    quads = sp // 4
    if paired and quads > 2:
        peers += [lax.rem(s + 4 * far, sp) for far in range(1, quads)]
    for peer in peers:
        pl.semaphore_signal(barrier, inc=1, device_id={"sp": peer}, device_id_type=MESH)
    for off in range(1, dp):
        pl.semaphore_signal(
            barrier, inc=1, device_id={"dp": lax.rem(d + off, dp)}, device_id_type=MESH
        )

    loads[0].wait()
    for load in loads[3:]:
        load.start()
    for load in loads[1:3]:
        load.wait()
    value_f, gate_f = dot(x[...], wv[...], NN), dot(x[...], wg[...], NN)
    value[...] = value_f.astype(BF16).astype(F32)
    opening[...] = gate_f.astype(BF16).astype(F32)

    def row_loop(fn, init=None, rows=ROWS, begin=0, end=tokens):
        def step(i, carry):
            return fn(pl.multiple_of(begin + i * rows, math.gcd(begin, rows)), carry)

        return lax.fori_loop(0, (end - begin) // rows, step, init)

    ext = tokens + 2 * PAD
    inner_rows = ext - 2 * ROWS
    big = 96 if inner_rows % 96 == 0 else ROWS
    own = pl.ds(PAD, tokens)

    def make_glu(r, _):
        here = pl.ds(r, ROWS)
        o = jax.nn.sigmoid(opening[here, :])
        opening[here, :] = o
        glu[pl.ds(r + 2 * PAD, ROWS), :] = value[here, :] * o

    row_loop(make_glu)
    pl.semaphore_wait(barrier, len(peers) + dp - 1)

    has_low, has_high = s > 0, s < sp - 1

    def halo_copies(buf, pad, at):
        up = pltpu.make_async_remote_copy(
            src_ref=buf.at[pl.ds(tokens, pad)],
            dst_ref=buf.at[pl.ds(0, pad)],
            send_sem=halo_send.at[at],
            recv_sem=halo_recv.at[at],
            device_id={"sp": lax.rem(s + 1, sp)},
            device_id_type=MESH,
        )
        down = pltpu.make_async_remote_copy(
            src_ref=buf.at[pl.ds(pad, pad)],
            dst_ref=buf.at[pl.ds(tokens + pad, pad)],
            send_sem=halo_send.at[at + 1],
            recv_sem=halo_recv.at[at + 1],
            device_id={"sp": lax.rem(s + sp - 1, sp)},
            device_id_type=MESH,
        )
        return up, down

    def halo_zero(buf, pad):
        @pl.when(s == 0)
        def _():
            buf[pl.ds(0, pad), :] = jnp.zeros((pad, chans), F32)

        @pl.when(s == sp - 1)
        def _():
            buf[pl.ds(tokens + pad, pad), :] = jnp.zeros((pad, chans), F32)

    def halo_start(buf, pad, at):
        up, down = halo_copies(buf, pad, at)
        pl.when(has_high)(up.start)
        pl.when(has_low)(down.start)
        halo_zero(buf, pad)

    def halo_wait(buf, pad, at):
        up, down = halo_copies(buf, pad, at)

        @pl.when(has_low)
        def _():
            up.wait_recv()
            down.wait_send()

        @pl.when(has_high)
        def _():
            down.wait_recv()
            up.wait_send()

    half = tokens // 2
    hand = chans // 2
    core = lax.rem(d, 2)
    these = pl.ds(pl.multiple_of(core * half, half), half)
    slots = [(far, other) for other in (1, 0) for far in range(quads)]
    held_rows, near_rows = (x, og), (xp, ogp)
    in_bits, mid_bits = (1, 0), (0, 1)

    def columns_of(who, far, other, kind):
        index = lax.rem(who + 4 * far, sp)
        if other:
            index = flip(index, mid_bits[kind])
        return pl.ds(pl.multiple_of(index * chunk, chunk), chunk)

    def slot_of(far, other):
        return pl.ds((2 * far + other) * chunk, chunk)

    def send_to(at, src, dst, recv_sem, where):
        return pltpu.make_async_remote_copy(
            src_ref=src,
            dst_ref=dst,
            send_sem=pair_sends.at[at],
            recv_sem=recv_sem,
            device_id=where,
            device_id_type=MESH,
        )

    def near_start(kind, those):
        there = flip(s, in_bits[kind])
        for far, other in those if paired else ():
            send_to(
                kind,
                held_rows[kind].at[these, columns_of(there, far, other, kind)],
                near_rows[kind].at[these, slot_of(far, other)],
                near_recv.at[kind],
                {"sp": there},
            ).start()

    def near_all(kind, stage):
        where = {"dp": flip(d, 0)} if stage else {"sp": flip(s, in_bits[kind])}
        rows = near_rows[kind].at[these]
        at = kind + 2 * stage
        return send_to(at, rows, rows, near_recv.at[at], where)

    halo_start(glu, 2 * PAD, 0)
    for load in loads[3:]:
        load.wait()
    d_act[own, :] = dot(og[...], wd[...], NT)
    halo_start(d_act, PAD, 2)

    span = ROWS + 2 * PAD

    def shifted(buf, r, offset):
        window = buf[pl.ds(r, span), :]
        return pltpu.roll(window, span - offset, 0) if offset else window

    def slide(buf, r, offset_of, acc):
        for low in range(8):
            those = [tap for tap in range(taps) if offset_of(tap) % 8 == low]
            if those:
                window = shifted(buf, r, low)
                for tap in those:
                    high = offset_of(tap) - low
                    acc = acc + ck[tap : tap + 1, :] * window[high : high + ROWS]
        return acc

    def conv(r, _):
        acc = jnp.zeros((ROWS, chans), F32) + bias[...]
        mixed[pl.ds(r, ROWS), :] = slide(glu, r, lambda tap: tap + PAD - reach, acc)

    ones = jnp.ones((16, chans), BF16)
    eye = (
        lax.rem(lax.broadcasted_iota(jnp.int32, (24, 128), 0), 8)
        == lax.broadcasted_iota(jnp.int32, (24, 128), 1)
    ).astype(BF16)
    edges = ((0, ROWS), (ext - ROWS, ROWS))
    regions = (((ROWS, inner_rows),), edges)

    def pieces_of(region):
        count = sum(size for _, size in regions[region])
        return [(at, min(128, count - at)) for at in range(0, count, 128)]

    def rows_of(buf, region):
        got = [buf[pl.ds(first, size), :] for first, size in regions[region]]
        return got[0] if len(got) == 1 else jnp.concatenate(got, axis=0)

    def row_sums(v):
        a, b, c = (dot(ones, term, NT) for term in split3(v))
        return a + b + c

    def columns(at, region, one, two):
        line = lax.broadcasted_iota(jnp.int32, (8, one.shape[1]), 0)
        both = jnp.where(line == 0, one, jnp.where(line == 1, two, 0.0))
        terms = [term.astype(F32) for term in split3(both)]
        got = dot(jnp.concatenate(terms, axis=0).astype(BF16), eye, TN)
        done = 0
        for first, size in regions[region]:
            cols[at, pl.ds(first, size), :] = got[done : done + size]
            done += size

    def stat_copy(at, off):
        return pltpu.make_async_remote_copy(
            src_ref=stats.at[at, 0],
            dst_ref=stats.at[at, off],
            send_sem=stat_send.at[at],
            recv_sem=stat_recv.at[at],
            device_id={"dp": lax.rem(d + off, dp)},
            device_id_type=MESH,
        )

    def stat_all(at):
        every = stats.at[at, pl.ds(1, dp - 1)]
        return pltpu.make_async_remote_copy(
            src_ref=every,
            dst_ref=every,
            send_sem=stat_send.at[at],
            recv_sem=stat_recv.at[at],
            device_id={"dp": lax.rem(d + 1, dp)},
            device_id_type=MESH,
        )

    def stat_start(at, region, one, two):
        pieces = pieces_of(region)
        stats[at, 0] = jnp.zeros(stats.shape[2:], F32)
        for first, sums in ((0, row_sums(one)), (len(pieces), row_sums(two))):
            for j, (begin, size) in enumerate(pieces):
                stats[at, 0, first + j : first + j + 1, 0:size] = sums[0:1, begin : begin + size]
        for off in range(1, dp):
            stat_copy(at, off).start()

    def stat_wait(at, region):
        pieces = pieces_of(region)
        stat_all(at).wait_recv()
        total = stats[at, 0]
        for off in range(1, dp):
            total = total + stats[at, off]
        total = total * (1.0 / channels)
        return tuple(
            jnp.concatenate(
                [total[first + j : first + j + 1, 0:size] for j, (_, size) in enumerate(pieces)],
                axis=1,
            )
            for first in (0, len(pieces))
        )

    def moments_start(region):
        v = rows_of(mixed, region)
        stat_start(region, region, v, v * v)

    def moments_wait(region):
        mean, square = stat_wait(region, region)
        columns(0, region, mean, lax.rsqrt(square - mean * mean + EPS))

    def second_start(region):
        v = rows_of(d_act, region)
        stat_start(2 + region, region, v, v * rows_of(mixed, region))

    def second_wait(region):
        columns(1, region, *stat_wait(2 + region, region))

    row_loop(conv, begin=ROWS, end=ext - ROWS)
    moments_start(0)
    halo_wait(glu, 2 * PAD, 0)
    near_start(1, slots)
    near_start(0, slots)

    def conv_edge(i, _):
        conv(pl.multiple_of(i * (ext - ROWS), ROWS), None)

    lax.fori_loop(0, 2, conv_edge, None)
    moments_start(1)

    def norm_rows(r, rows):
        here = pl.ds(r, rows)
        col = cols[0, here, :]
        centred = (mixed[here, :] - col[:, 0:1]) * col[:, 1:2]
        normed = centred * gain[...] + shift[...]
        sig = jax.nn.sigmoid(normed)
        act[here, :] = (normed * sig).astype(BF16)
        d_normed = d_act[here, :] * sig * (1.0 + normed * (1.0 - sig))
        mixed[here, :] = centred
        d_act[here, :] = d_normed * gain[...]
        return d_normed * centred, d_normed

    def down(v):
        return jnp.sum(v, axis=0, keepdims=True)

    def norm(r, carry):
        return tuple(had + down(v) for had, v in zip(carry, norm_rows(r, big)))

    zero = jnp.zeros((1, chans), F32)
    moments_wait(0)
    sums = row_loop(norm, (zero, zero), big, ROWS, ext - ROWS)
    second_start(0)
    halo_wait(d_act, PAD, 2)
    moments_wait(1)
    kept = (slice(PAD, ROWS), slice(0, ROWS - PAD))
    for (first, size), keep in zip(edges, kept):
        sums = tuple(had + down(v[keep]) for had, v in zip(sums, norm_rows(first, size)))
    gain_sum, shift_sum = sums
    second_start(1)

    def several(count, fn):
        if count <= 8:
            for i in range(count):
                fn(i)
        else:
            lax.fori_loop(0, count, lambda i, _: fn(i), None)

    def grad_tile(at, rows, off):
        index = index_of(lax.rem(pos + off + 2 * sp, sp))
        those = pl.ds(pl.multiple_of(index * chunk, chunk), chunk)
        part[at, pl.ds(pl.multiple_of(index * lines, lines), lines), :] = dot(
            turned[at], rows[:, those], NN
        )

    def grad_first(at, rows, factor):
        if wide:
            turned[at] = factor.T
            grad_tile(at, rows, -1)
            grad_tile(at, rows, 1)
            return

        def step(i, _):
            here = pl.ds(pl.multiple_of(i * tile, tile), tile)
            part[at, here, :] = dot(rows[:, here], factor, TN)

        lax.fori_loop(0, width // tile, step, None)

    def grad_rest(at, rows):
        if wide:
            several(sp - 2, lambda i: grad_tile(at, rows, (i + 2) % (sp - 1)))

    streams = [
        (at, 2 * sub + (way < 0), way) for at in range(3) for sub in range(SUBS) for way in (1, -1)
    ]
    early = [i for i, (at, _, _) in enumerate(streams) if at == 2]
    late = [i for sub in range(SUBS) for i, (at, place, _) in enumerate(streams) if at < 2 and place // 2 == sub]

    def late_of(at):
        return [i for i in late if streams[i][0] == at]

    def piece(stream, p):
        at, place, _ = streams[stream]
        first = index_of(lax.rem(p + 2 * sp, sp)) * lines + place * strip
        return part[at, pl.ds(pl.multiple_of(first, strip), strip), :]

    def ring_copy(stream, k):
        return pltpu.make_async_remote_copy(
            src_ref=ring_src.at[stream, k],
            dst_ref=ring_dst.at[stream, k],
            send_sem=ring_send.at[0],
            recv_sem=ring_recv.at[stream, k],
            device_id={"sp": ahead if streams[stream][2] == 1 else behind},
            device_id_type=MESH,
        )

    def ring_step(k, which):
        for stream in which:
            way = streams[stream][2]
            mine = piece(stream, pos - way * (1 + k))
            if not (isinstance(k, int) and k == 0):
                ring_copy(stream, k - 1).wait_recv()
                mine = mine + ring_dst[stream, k - 1].astype(F32)
            ring_src[stream, k] = mine.astype(BF16)
            ring_copy(stream, k).start()

    def ring_end(which, outs):
        for stream in which:
            at, place, _ = streams[stream]
            ring_copy(stream, sp - 2).wait_recv()
            outs[at][pl.ds(place * strip, strip), :] = ratio * (
                piece(stream, pos) + ring_dst[stream, sp - 2].astype(F32)
            )

    blocks = [(at, hand * place) for at in (2, 0, 1) for place in range(2)]

    def kind_of(n):
        return int(blocks[n][0] == 2)

    def factor_of(n):
        at, first = blocks[n]
        those = pl.ds(first, hand)
        return (dv, dg, act)[at].at[own if at == 2 else pl.ds(0, tokens), those]

    def in_copy(n):
        where = {"sp": flip(s, in_bits[kind_of(n)])}
        return send_to(4, factor_of(n), in_recv.at[n], in_rsem.at[n], where)

    strips = [pl.ds(cut * (hand // CUTS), hand // CUTS) for cut in range(CUTS)]

    def mid_copy(n, cut):
        where = {"sp": flip(s, mid_bits[kind_of(n)])}
        at, far = (7, 0) if n in DIRECT else (5, slice(None))
        src, dst = x_send.at[n, far, strips[cut]], x_recv.at[n, far, strips[cut]]
        return send_to(at, src, dst, x_rsem.at[n, cut], where)

    def cross_copy(n, far):
        at = DIRECT.index(n)
        where = {"sp": flip(lax.rem(s + 4 * far, sp), mid_bits[kind_of(n)])}
        return send_to(
            8, z_send2.at[at, far - 1], z_recv2.at[at, far - 1], cross_rsem.at[at, far - 1], where
        )

    def far_copy(n, far, cut):
        where = {"sp": lax.rem(s + 4 * far, sp)}
        src, dst = z_send.at[n, far - 1, strips[cut]], z_recv.at[n, far - 1, strips[cut]]
        return send_to(6, src, dst, z_rsem.at[n, far - 1, cut], where)

    def far_copies(n, far):
        return [far_copy(n, far, cut) for cut in range(CUTS)]

    def product(n):
        kind = kind_of(n)
        in_copy(n).wait_recv()
        lhs[...] = jnp.concatenate([factor_of(n)[...], in_recv[n]], axis=0).T
        direct = n in DIRECT
        for far, other in sorted(slots, key=lambda at: -at[0]) if direct else slots:
            mine = held_rows[kind][:, columns_of(s, far, other, kind)]
            rows = jnp.concatenate([mine, near_rows[kind][:, slot_of(far, other)]], axis=0)
            got = dot(lhs[...], rows, NN)
            if direct and far:
                sent = got.astype(BF16)
                if other:
                    z_send2[DIRECT.index(n), far - 1] = sent
                else:
                    z_send[n, far - 1] = sent
                for copy in [cross_copy(n, far)] if other else far_copies(n, far):
                    copy.start()
            elif other:
                x_send[n, far] = got.astype(BF16)
            else:
                held[n, far] = got
            if (far, other) == (0 if direct else quads - 1, 1):
                for cut in range(CUTS):
                    mid_copy(n, cut).start()

    def meet(n):
        for cut, rows in enumerate(strips):
            mid_copy(n, cut).wait_recv()
            for far in () if n in DIRECT else range(1, quads):
                got = held[n, far, rows, :] + x_recv[n, far, rows, :].astype(F32)
                z_send[n, far - 1, rows, :] = got.astype(BF16)
                far_copy(n, far, cut).start()
            held[n, 0, rows, :] = held[n, 0, rows, :] + x_recv[n, 0, rows, :].astype(F32)

    def settle(n, outs):
        at, first = blocks[n]
        total = held[n, 0]
        for far in range(1, quads):
            for copy in far_copies(n, far):
                copy.wait_recv()
            total = total + z_recv[n, far - 1].astype(F32)
            if n in DIRECT:
                cross_copy(n, far).wait_recv()
                total = total + z_recv2[DIRECT.index(n), far - 1].astype(F32)
        outs[at][pl.ds(first, hand), :] = ratio * total

    if paired:
        for n in range(2):
            in_copy(n).start()
    else:
        grad_first(2, og, act[own, :])
        ring_step(0, early)
        grad_rest(2, og)

    def back_rows(r, rows):
        here = pl.ds(r, rows)
        col, back = cols[0, here, :], cols[1, here, :]
        d_mixed = col[:, 1:2] * (d_act[here, :] - back[:, 0:1] - mixed[here, :] * back[:, 1:2])
        d_pad[here, :] = d_mixed
        return d_mixed

    def norm_back(r, bias_sum):
        return bias_sum + down(back_rows(r, big))

    def conv_back(r, _):
        here = pl.ds(r, ROWS)
        acc = jnp.zeros((ROWS, chans), F32)
        acc = slide(d_pad, r, lambda tap: PAD + reach - tap, acc)
        o = opening[here, :]
        grad = acc * o
        dv[here, :] = grad.astype(BF16)
        dg[here, :] = (grad * value[here, :] * (1.0 - o)).astype(BF16)

    second_wait(0)
    bias_sum = row_loop(norm_back, zero, big, ROWS, ext - ROWS)
    row_loop(conv_back, begin=ROWS, end=tokens - ROWS)
    second_wait(1)
    for (first, size), keep in zip(edges, kept):
        bias_sum = bias_sum + down(back_rows(first, size)[keep])
    halo_zero(d_pad, PAD)

    def back_edge(i, _):
        conv_back(pl.multiple_of(i * (tokens - ROWS), ROWS), None)

    lax.fori_loop(0, 2, back_edge, None)
    if not paired:
        ring_step(1, early)
    if paired:
        for n in range(2, 6):
            in_copy(n).start()
    else:
        grad_first(0, x, dv[...])
        ring_step(0, late_of(0))
        grad_first(1, x, dg[...])
        ring_step(0, late_of(1))
        grad_rest(0, x)
        grad_rest(1, x)
        ring_step(2, early)

    mine = pl.multiple_of(lax.rem(d, 2) * half, half)
    other = pl.multiple_of((1 - lax.rem(d, 2)) * half, half)
    group = width // GROUPS

    def ig_copy(at, g, src, dst, bit):
        return pltpu.make_async_remote_copy(
            src_ref=src,
            dst_ref=dst,
            send_sem=ig_ssem.at[at],
            recv_sem=give_rsem.at[0] if at == bits_dp else ig_rsem.at[at, g],
            device_id={"dp": flip(d, bit)},
            device_id_type=MESH,
        )

    def of_group(g):
        return pl.ds(g * group, group)

    def pair_copy(g):
        return ig_copy(0, g, ig_send.at[:, of_group(g)], ig_recv.at[:, of_group(g)], 0)

    def y_copy(bit, g):
        return ig_copy(
            bit, g, ig_sum.at[bit - 1, :, of_group(g)], ig_peer.at[bit - 1, :, of_group(g)], bit
        )

    final = bits_dp - 1

    def give_copy(g):
        return ig_copy(
            bits_dp,
            g,
            ig_sum.at[final, :, of_group(g)],
            ig_out.at[pl.ds(mine, half), of_group(g)],
            0,
        )

    small[0] = jnp.zeros(small.shape[1:], F32)

    def taps_grad(low):
        those = [
            [tap for tap in range(taps) if (tap + PAD - reach) % 8 == low + at] for at in range(2)
        ]

        def taps_sum(r, sums):
            grad = d_pad[pl.ds(r + PAD, ROWS), :]
            new = []
            for at in range(2):
                window = shifted(glu, r + PAD, low + at)
                for tap in those[at]:
                    high = tap + PAD - reach - low - at
                    prod = grad * window[high : high + ROWS]
                    acc = sums[len(new)]
                    for row in range(0, ROWS, 8):
                        acc = acc + prod[row : row + 8]
                    new.append(acc)
            return tuple(new)

        flat = those[0] + those[1]
        sums = row_loop(taps_sum, tuple(jnp.zeros((8, chans), F32) for _ in flat))
        for acc, tap in zip(sums, flat):
            small[0, tap : tap + 1, :] = jnp.sum(acc, axis=0, keepdims=True) * ratio

    part_rows = small.shape[1] // 2
    my_rows = pl.ds(pl.multiple_of(lax.rem(s, 2) * part_rows, 8), part_rows)

    def small_copy(turn):
        if turn == 0:
            src, dst, bit = small.at[0], small_recv.at[0], 0
        elif turn < bits_sp:
            src, dst, bit = small.at[turn, my_rows], small_recv.at[turn, my_rows], turn
        else:
            src, dst, bit = small.at[turn, my_rows], small.at[turn, my_rows], 0
        return pltpu.make_async_remote_copy(
            src_ref=src,
            dst_ref=dst,
            send_sem=small_ssem.at[min(turn, 1)],
            recv_sem=small_rsem.at[turn],
            device_id={"sp": flip(s, bit)},
            device_id_type=MESH,
        )

    def small_first():
        small[0, taps : taps + 1, :] = bias_sum * ratio
        small[0, taps + 1 : taps + 2, :] = gain_sum * ratio
        small[0, taps + 2 : taps + 3, :] = shift_sum * ratio
        small_copy(0).start()

    def small_next(turn):
        small_copy(turn).wait_recv()
        if turn < bits_sp:
            those = my_rows if turn else slice(None)
            small[turn + 1, those, :] = small[turn, those, :] + small_recv[turn, those, :]
            small_copy(turn + 1).start()

    def taps_half(lows):
        for low in lows:
            taps_grad(low)

    both_v = jnp.concatenate([dv[pl.ds(other, half), :], dv[pl.ds(mine, half), :]], axis=0)
    both_g = jnp.concatenate([dg[pl.ds(other, half), :], dg[pl.ds(mine, half), :]], axis=0)
    size = min(tile, group)
    for g in range(GROUPS):
        for begin in range(g * group, (g + 1) * group, size):
            here = pl.ds(begin, size)
            got = dot(both_v, wv[here, :], NT) + dot(both_g, wg[here, :], NT)
            ig_send[:, here] = got[:half].astype(BF16)
            ig_own[:, here] = got[half:]
        pair_copy(g).start()

    def pair_sums():
        for g in range(GROUPS):
            pair_copy(g).wait_recv()
            here = of_group(g)
            ig_sum[0, :, here] = (ig_own[:, here] + ig_recv[:, here].astype(F32)).astype(BF16)
            if bits_dp > 1:
                y_copy(1, g).start()

    if paired:
        for kind in (1, 0):
            near_all(kind, 0).wait_recv()
            near_all(kind, 1).start()
        taps_half((0, 2, 4, 6))
        small_first()
    pair_sums()
    fixed = min(sp - 2, 6)
    if paired:
        near_all(0, 1).wait_recv()
        product(2)
        product(3)
        small_next(0)
        near_all(1, 1).wait_recv()
        product(0)
        product(1)
        product(4)
        product(5)
        small_next(1)
        meet(2)
        meet(3)
        meet(0)
        meet(4)
        meet(1)
        meet(5)
        small_next(2)
        for turn in range(3, bits_sp + 1):
            small_next(turn)
        fixed = 0
    for k in range(1, fixed + 1):
        ring_step(k, late)
        if k + 2 <= sp - 2:
            ring_step(k + 2, early)
        if k == 1:
            taps_half((0, 2))
        if k == 2:
            taps_half((4, 6))
            small_first()
        if k > 2 and k - 3 <= bits_sp:
            small_next(k - 3)
    for turn in range(max(fixed - 2, 0), bits_sp + 1 if fixed else 0):
        small_next(turn)
    if sp - 2 > fixed and fixed:

        def both(k, _):
            ring_step(k, late)
            ring_step(k + 2, early)

        lax.fori_loop(fixed + 1, sp - 3, both, None)
        ring_step(sp - 3, late)
        ring_step(sp - 2, late)

    for bit in range(1, bits_dp):
        for g in range(GROUPS):
            y_copy(bit, g).wait_recv()
            here = of_group(g)
            got = ig_sum[bit - 1, :, here].astype(F32) + ig_peer[bit - 1, :, here].astype(F32)
            ig_sum[bit, :, here] = got.astype(BF16)
            if bit + 1 < bits_dp:
                y_copy(bit + 1, g).start()
            else:
                give_copy(g).start()
    if bits_dp == 1:
        for g in range(GROUPS):
            give_copy(g).start()
    ig_out[pl.ds(mine, half), :] = ig_sum[final]
    small_out[...] = small[bits_sp]
    if paired:
        for n in (2, 3, 0, 4, 1, 5):
            settle(n, (vg_out, gg_out, dg_out))
        for kind in range(2):
            near_all(kind, 0).wait_send()
            near_all(kind, 1).wait_send()
        waits = [(4, in_recv), (5, x_send.at[pl.ds(0, 6 - len(DIRECT))]), (6, z_send)]
        if DIRECT:
            waits += [(7, x_send.at[pl.ds(0, len(DIRECT)), 0]), (8, z_send2)]
        for at, ref in waits:
            send_to(at, ref, ref, near_recv.at[0], {"sp": flip(s, 0)}).wait_send()
    else:
        ring_end(early + late, (vg_out, gg_out, dg_out))
        pltpu.make_async_remote_copy(
            src_ref=ring_src,
            dst_ref=ring_dst,
            send_sem=ring_send.at[0],
            recv_sem=ring_recv.at[0, 0],
            device_id={"sp": ahead},
            device_id_type=MESH,
        ).wait_send()

    ig_copy(0, 0, ig_send, ig_recv, 0).wait_send()
    for bit in range(1, bits_dp):
        ig_copy(bit, 0, ig_sum.at[bit - 1], ig_peer.at[bit - 1], bit).wait_send()
    ig_copy(bits_dp, 0, ig_sum.at[final], ig_out.at[pl.ds(mine, half)], 0).wait()
    for at in range(4):
        stat_all(at).wait_send()
    for at, sent in ((0, small.at[0]), (1, small.at[pl.ds(1, bits_sp), my_rows])):
        pltpu.make_async_remote_copy(
            src_ref=sent,
            dst_ref=sent,
            send_sem=small_ssem.at[at],
            recv_sem=small_rsem.at[0],
            device_id={"sp": flip(s, 0)},
            device_id_type=MESH,
        ).wait_send()


def finish(
    wide, ig, vg, gg, dgrad, small, ig_o, vg_o, gg_o, dg_o, k_o, b_o, g_o, s_o,
    t0, t1, k_v, b_v, g_v, s_v, sem,
):
    copies = []

    def send(src, dst):
        copies.append(pltpu.make_async_copy(src, dst, sem.at[len(copies)]))
        copies[-1].start()

    send(ig, ig_o)
    turn = [(vg, vg_o), (gg, gg_o)] if wide else [(dgrad, dg_o)]
    keep = [(dgrad, dg_o)] if wide else [(vg, vg_o), (gg, gg_o)]
    for src, dst in keep:
        send(src, dst)
    taps = k_o.shape[0]
    k_v[...] = small[0:taps, :]
    send(k_v, k_o)
    for at, (held, out) in enumerate(((b_v, b_o), (g_v, g_o), (s_v, s_o))):
        held[...] = small[taps + at, :]
        send(held, out)
    for (src, dst), held in zip(turn, (t0, t1)):
        held[...] = src[...].T
        send(held, dst)
    for copy in copies:
        copy.wait()


def on_device(
    normed_input,
    out_grad,
    value_weight,
    gate_weight,
    down_weight,
    conv_kernel,
    conv_bias,
    norm_gain,
    norm_shift,
):
    tokens, width = normed_input.shape
    taps, chans = conv_kernel.shape
    sp, dp = lax.axis_size("sp"), lax.axis_size("dp")
    ratio = 1.0 / math.sqrt(tokens * sp)
    chunk = width // sp
    bits_sp, bits_dp = sp.bit_length() - 1, dp.bit_length() - 1
    small_rows = -(-(taps + 3) // 16) * 16
    half = tokens // 2
    full, extended = (tokens, chans), (tokens + 2 * PAD, chans)
    vmem = pl.BlockSpec(memory_space=pltpu.VMEM)
    hbm = pl.BlockSpec(memory_space=pltpu.HBM)
    dma = pltpu.SemaphoreType.DMA
    wide = is_wide(chunk, chans)
    lines, lanes = (chans, chunk) if wide else (chunk, chans)
    stat_rows = -(-2 * -(-tokens // 128) // 8) * 8
    paired = is_paired(sp, dp, chunk, chans)
    if paired:
        ring_shape, ring_sems, part_shape, turned_shape = (1, 1, 16, 128), (1, 1), (1, 8, 128), (1, 16, 128)
    else:
        count = 3 * 2 * SUBS
        ring_shape, ring_sems = (count, sp - 1, lines // (2 * SUBS), lanes), (count, sp - 1)
        part_shape, turned_shape = (3, sp * lines, lanes), (3, chans, tokens)
    quads, hand = (sp // 4, chans // 2) if paired else (2, 16)
    near, wide_chunk = (tokens, chunk) if paired else (16, 128)
    pair_scratch = [
        pltpu.VMEM((near, 2 * quads * wide_chunk), BF16),
        pltpu.VMEM((near, 2 * quads * wide_chunk), BF16),
        pltpu.VMEM((6, near, hand), BF16),
        pltpu.VMEM((hand, 2 * near), BF16),
        pltpu.VMEM((6, quads, hand, wide_chunk), BF16),
        pltpu.VMEM((6, quads, hand, wide_chunk), BF16),
        pltpu.VMEM((6, quads, hand, wide_chunk), F32),
        pltpu.VMEM((6, quads - 1, hand, wide_chunk), BF16),
        pltpu.VMEM((6, quads - 1, hand, wide_chunk), BF16),
        pltpu.VMEM((max(len(DIRECT), 1), quads - 1, hand, wide_chunk), BF16),
        pltpu.VMEM((max(len(DIRECT), 1), quads - 1, hand, wide_chunk), BF16),
        pltpu.SemaphoreType.DMA((9,)),
        pltpu.SemaphoreType.DMA((4,)),
        pltpu.SemaphoreType.DMA((6,)),
        pltpu.SemaphoreType.DMA((6, CUTS)),
        pltpu.SemaphoreType.DMA((6, quads - 1, CUTS)),
        pltpu.SemaphoreType.DMA((max(len(DIRECT), 1), quads - 1)),
    ]
    ig, vg, gg, dgrad, small = pl.pallas_call(
        functools.partial(kernel, sp, dp, ratio),
        out_shape=(
            pltpu.VMEM((tokens, width), BF16),
            pltpu.VMEM((lines, lanes), F32),
            pltpu.VMEM((lines, lanes), F32),
            pltpu.VMEM((lines, lanes), F32),
            pltpu.VMEM((small_rows, chans), F32),
        ),
        in_specs=[hbm] * 9,
        out_specs=(vmem,) * 5,
        scratch_shapes=[
            pltpu.VMEM((tokens, width), BF16),
            pltpu.VMEM((tokens, width), BF16),
            pltpu.VMEM((width, chans), BF16),
            pltpu.VMEM((width, chans), BF16),
            pltpu.VMEM((chans, width), BF16),
            pltpu.VMEM((taps, chans), F32),
            pltpu.VMEM((1, chans), F32),
            pltpu.VMEM((1, chans), F32),
            pltpu.VMEM((1, chans), F32),
            dma((9,)),
            pltpu.VMEM(full, F32),
            pltpu.VMEM(full, F32),
            pltpu.VMEM((tokens + 4 * PAD, chans), F32),
            pltpu.VMEM(extended, F32),
            pltpu.VMEM(extended, F32),
            pltpu.VMEM(extended, F32),
            pltpu.VMEM(extended, BF16),
            pltpu.VMEM(full, BF16),
            pltpu.VMEM(full, BF16),
            pltpu.VMEM(turned_shape, BF16),
            pltpu.VMEM((2, tokens + 2 * PAD, 128), F32),
            pltpu.VMEM((4, dp, stat_rows, 128), F32),
            pltpu.VMEM(part_shape, F32),
            pltpu.VMEM(ring_shape, BF16),
            pltpu.VMEM(ring_shape, BF16),
            pltpu.VMEM((half, width), BF16),
            pltpu.VMEM((half, width), BF16),
            pltpu.VMEM((half, width), F32),
            pltpu.VMEM((bits_dp, half, width), BF16),
            pltpu.VMEM((bits_dp - 1, half, width), BF16),
            pltpu.VMEM((bits_sp + 1, small_rows, chans), F32),
            pltpu.VMEM((bits_sp, small_rows, chans), F32),
            dma((4,)),
            dma((4,)),
            dma((4,)),
            dma((4,)),
            dma((1,)),
            dma(ring_sems),
            dma((bits_dp + 1,)),
            dma((bits_dp, GROUPS)),
            dma((1,)),
            dma((2,)),
            dma((bits_sp + 1,)),
            *pair_scratch,
        ],
        compiler_params=pltpu.CompilerParams(
            collective_id=0, has_side_effects=True, vmem_limit_bytes=MAIN
        ),
    )(
        normed_input,
        out_grad,
        value_weight,
        gate_weight,
        down_weight,
        conv_kernel,
        conv_bias[None, :],
        norm_gain[None, :],
        norm_shift[None, :],
    )
    row = jax.ShapeDtypeStruct((chans,), F32)
    return pl.pallas_call(
        functools.partial(finish, wide),
        out_shape=(
            jax.ShapeDtypeStruct(ig.shape, BF16),
            jax.ShapeDtypeStruct(vg.shape, F32),
            jax.ShapeDtypeStruct(gg.shape, F32),
            jax.ShapeDtypeStruct((chans, chunk), F32),
            jax.ShapeDtypeStruct((taps, chans), F32),
            row,
            row,
            row,
        ),
        in_specs=[vmem] * 5,
        out_specs=(hbm,) * 8,
        scratch_shapes=[
            pltpu.VMEM((lanes, lines), F32),
            pltpu.VMEM((lanes, lines), F32),
            pltpu.VMEM((taps, chans), F32),
            pltpu.VMEM((chans,), F32),
            pltpu.VMEM((chans,), F32),
            pltpu.VMEM((chans,), F32),
            dma((8,)),
        ],
        compiler_params=pltpu.CompilerParams(vmem_limit_bytes=FINISH),
    )(ig, vg, gg, dgrad, small)


def solution(mesh):
    in_specs = (
        P("sp", None),
        P("sp", None),
        P(None, "dp"),
        P(None, "dp"),
        P("dp", None),
        P(None, "dp"),
        P("dp"),
        P("dp"),
        P("dp"),
    )
    out_specs = (
        P("sp", None),
        P("sp", "dp"),
        P("sp", "dp"),
        P("dp", "sp"),
        P(None, "dp"),
        P("dp"),
        P("dp"),
        P("dp"),
    )
    return jax.shard_map(
        on_device, mesh=mesh, in_specs=in_specs, out_specs=out_specs, check_vma=False
    )
```
